128 devices in a mesh: ep: 32 (over z, y, core), tp: 4 (over x).
Axes of the slice: x: 4, y: 4, z: 4, core: 2. Of those that a mesh axis runs over, the one named last changes fastest.
Arguments:
- queries: bfloat16 [65536, 1024], P('ep', 'tp'), may hold values from -6 to 6
- keys_values: bfloat16 [65536, 512], P('ep', 'tp'), may hold values from -6 to 6
- sink_logits: float32 [16], replicated, may hold values from 4 to 8
- out_weight: bfloat16 [1024, 2048], replicated, may hold values from -4 to 4
- expert_tokens: bfloat16 [32768, 2048], P(('ep', 'tp')), may hold values from -6 to 6
- norm_gain: float32 [2048], replicated, may hold values from 0.1 to 1.9
- routes: int32 [32768, 2], P(('ep', 'tp')), may hold values from 0 to 31, all different within a row; in each aligned block of 256 rows (0 to 255, 256 to 511, ...) at most 24 rows name the same one
- route_weights: float32 [32768, 2], P(('ep', 'tp')), may hold values from 0.1 to 1
- gate_weight: bfloat16 [32, 2048, 1024], P('ep', None, 'tp'), may hold values from -0.125 to 0.125
- up_weight: bfloat16 [32, 2048, 1024], P('ep', None, 'tp'), may hold values from -0.125 to 0.125
- down_weight: bfloat16 [32, 1024, 2048], P('ep', 'tp'), may hold values from -0.1875 to 0.1875
Outputs:
- mixer_out: bfloat16 [65536, 2048], P(('ep', 'tp'))
- expert_out: bfloat16 [32768, 2048], P(('ep', 'tp'))
The draws below stay inside these ranges and needn't reach their ends.
Inputs may be any that keep to these rules, and one draw needn't show every extreme that they name: `routes`: each row names 2 different experts. In each aligned block of 256 rows, no expert is named by more than 24 rows, and in some block an expert is named by exactly 24 rows.
All inputs are finite; a program needn't handle non-finite values.
Results may differ from the reference program's by a relative error of at most 0.012.
Values may be sent and summed in bfloat16 or wider, within the bound.
A program may use at most 128 MiB of HBM per device.

```python
import math
import jax
import jax.numpy as jnp
import numpy as np
from jax import lax

D = 2048
HEADS = 16
KV_HEADS = 4
GROUP = 4
HEAD_DIM = 64
WINDOW = 128
FE = 1024
TOPK = 2
MOE_ROWS = 256
SEQ = 65536
MOE_TOKENS = 32768
EXPERTS = 32
CAP = 24
N_TP = 4


def draw_queries(key, part):
    noise_key = jax.random.fold_in(key, 11)
    return jax.random.truncated_normal(noise_key, -6.0, 6.0, (SEQ, HEADS * HEAD_DIM)).astype(jnp.bfloat16)


def draw_keys_values(key, part):
    noise_key = jax.random.fold_in(key, 17)
    return jax.random.truncated_normal(noise_key, -6.0, 6.0, (SEQ, KV_HEADS * 2 * HEAD_DIM)).astype(jnp.bfloat16)


def block_scale(key, shape, split, least, high):
    level = 1.0
    for axis_at, shards_of in split:
        draws = jax.random.uniform(jax.random.fold_in(jax.random.fold_in(key, 6), axis_at), (shards_of,), jnp.float32, least / len(split), high / len(split))
        level = level * jnp.repeat(jnp.exp(draws), shape[axis_at] // shards_of).reshape((-1,) + (1,) * (len(shape) - 1 - axis_at))
    return level


def routed_block(own_key, own, number, rows, number_of, top, most, lean):
    order = jax.random.permutation(own_key, number_of)
    crowded, usual = portions_of(number_of, rows * top, most, lean, True), portions_of(number_of, rows * top, most, lean, False)
    places = jnp.arange(number_of)

    def named(lengths, rotation):
        used = int((lengths > 0).sum())
        fixed = max(1, used // 4)
        moved = fixed + (places - fixed + rotation * (used - fixed)) % max(1, number_of - fixed)
        return jnp.zeros((number_of,), jnp.int32).at[order[jnp.where(places < fixed, places, moved)]].set(jnp.asarray(lengths, jnp.int32))

    lengths = jnp.where(number % 4 == 0, named(crowded, number // 4), named(usual, number - number // 4 - 1))
    mixed = jax.random.permutation(jax.random.fold_in(own, 3), number_of)
    giver, taker = mixed[0:number_of // 2 * 2:2], mixed[1:number_of // 2 * 2:2]
    margin = jnp.minimum(lengths[giver] - 1, most - lengths[taker]) // 2
    margin = jnp.where((giver == order[0]) | (taker == order[0]) | (lengths[taker] == 0), 0, jnp.maximum(margin, 0))
    moved = jax.random.randint(jax.random.fold_in(own, 4), (number_of // 2,), 0, 1 << 20) % (margin + 1)
    lengths = lengths.at[giver].add(-moved).at[taker].add(moved)
    items = jnp.searchsorted(jnp.cumsum(lengths), jnp.arange(rows * top), side="right").astype(jnp.int32)
    table = items.reshape(top, rows).T
    table = table[jax.random.permutation(jax.random.fold_in(own, 1), rows)]
    rotation = jax.random.randint(jax.random.fold_in(own, 2), (rows, 1), 0, top)
    return jnp.take_along_axis(table, (jnp.arange(top)[None, :] + rotation) % top, axis=1)


def portions_of(number_of, total, most, skew, full):
    portions = [(1 << 20) // math.isqrt(grade ** skew) + 1 for grade in range(1, number_of + 1)]
    largest = most if full else min(most, max(-(-total // number_of), total * portions[0] // sum(portions)))
    least = 1 if total - largest >= number_of - 1 else 0
    counts, surplus = [largest] + [least] * (number_of - 1), total - largest - least * (number_of - 1)
    while surplus > 0:
        candidates = [i for i in range(1, number_of) if counts[i] < largest] or [i for i in range(1, number_of) if counts[i] < most]
        whole, left = sum([portions[i] for i in candidates]), surplus
        for i in candidates:
            addition = min(most - counts[i], max(1, left * portions[i] // whole), surplus)
            counts[i] = counts[i] + addition
            surplus = surplus - addition
    return np.array(counts)


def normal_values(rng, dims, width, limit, cuts=(), kind=jnp.bfloat16):
    result = width * jax.random.normal(rng, dims, jnp.float32)
    if cuts:
        result = result * block_scale(rng, dims, cuts, -0.22, 0.18)
    return jnp.clip(result, -limit, limit).astype(kind)


def setup_inputs(seed: int = 0) -> dict:
    keys = jax.random.split(jax.random.key(seed), 12)
    queries = draw_queries(jax.random.fold_in(keys[11], 71), 0)
    keys_values = draw_keys_values(jax.random.fold_in(keys[11], 71), 0)
    sink_logits = jnp.clip(jax.random.uniform(keys[2], (HEADS,), jnp.float32, 4.0, 8.0), 4.0, 8.0)
    out_weight = normal_values(keys[3], (HEADS * HEAD_DIM, D), 0.8, 4.0)
    expert_tokens = normal_values(keys[4], (MOE_TOKENS, D), 1.0, 6.0, ((0, 128),))
    norm_gain = jnp.clip(1.0 + 0.18 * jax.random.normal(keys[5], (D,), jnp.float32), 0.1, 1.9)
    routes_keys = jax.random.split(jax.random.fold_in(keys[6], 1), MOE_TOKENS // MOE_ROWS)
    routes_turns = jax.random.permutation(jax.random.fold_in(keys[6], 3), MOE_TOKENS // MOE_ROWS)
    routes = jax.vmap(lambda own, number: routed_block(jax.random.fold_in(keys[6], 2), own, number, MOE_ROWS, EXPERTS, TOPK, CAP, 2))(routes_keys, routes_turns).reshape((MOE_TOKENS, TOPK))
    route_weights = jnp.clip(0.1 + 0.9 * jax.random.uniform(keys[7], (MOE_TOKENS, TOPK), jnp.float32) ** block_scale(keys[7], (MOE_TOKENS, TOPK), ((0, 128),), -0.2, 0.2), 0.1, 1.0)
    gate_weight = normal_values(keys[8], (EXPERTS, D, FE), D ** -0.5, 0.125, ((0, 32), (2, 4)))
    up_weight = normal_values(keys[9], (EXPERTS, D, FE), D ** -0.5, 0.125, ((0, 32), (2, 4)))
    down_weight = normal_values(keys[10], (EXPERTS, FE, D), FE ** -0.5, 0.1875, ((0, 32), (1, 4)))
    return dict(queries=queries, keys_values=keys_values, sink_logits=sink_logits, out_weight=out_weight, expert_tokens=expert_tokens, norm_gain=norm_gain, routes=routes, route_weights=route_weights, gate_weight=gate_weight, up_weight=up_weight, down_weight=down_weight)


NEG_FILL = -1e+30

def attend_all(queries, keys_values, sink_logits):
    seq_total = queries.shape[0]
    block_rows = min(512, seq_total)
    key_span = block_rows + 2 * WINDOW
    query_all = queries.astype(jnp.float32).reshape(seq_total, KV_HEADS, GROUP, HEAD_DIM)
    pair_all = keys_values.astype(jnp.float32).reshape(seq_total, KV_HEADS, 2, HEAD_DIM)
    padded = jnp.pad(pair_all, ((WINDOW, WINDOW), (0, 0), (0, 0), (0, 0)))
    sink_grid = sink_logits.astype(jnp.float32).reshape(KV_HEADS, GROUP, 1, 1)

    def one_block(block_index):
        first_row = block_index * block_rows
        query_block = lax.dynamic_slice_in_dim(query_all, first_row, block_rows, 0)
        pair_block = lax.dynamic_slice_in_dim(padded, first_row, key_span, 0)
        scores = jnp.einsum('qhgd,khd->hgqk', query_block, pair_block[:, :, 0]) * HEAD_DIM ** (-0.5)
        query_pos = first_row + jnp.arange(block_rows, dtype=jnp.int32)
        key_pos = first_row - WINDOW + jnp.arange(key_span, dtype=jnp.int32)
        allowed = (jnp.abs(query_pos[:, None] - key_pos[None, :]) <= WINDOW) & (key_pos >= 0)[None, :] & (key_pos < seq_total)[None, :]
        scores = jnp.where(allowed, scores, NEG_FILL)
        top_score = jnp.maximum(lax.optimization_barrier(jnp.max(scores, -1, keepdims=True)), sink_grid)
        exp_scores = jnp.exp(scores - top_score)
        denominator = lax.optimization_barrier(jnp.sum(exp_scores, -1, keepdims=True)) + jnp.exp(sink_grid - top_score)
        attn_weights = lax.optimization_barrier((exp_scores / denominator).astype(jnp.bfloat16)).astype(jnp.float32)
        head_values = jnp.einsum('hgqk,khd->qhgd', attn_weights, pair_block[:, :, 1])
        return head_values.astype(jnp.bfloat16).reshape(block_rows, HEADS * HEAD_DIM)
    blocks = lax.map(one_block, jnp.arange(seq_total // block_rows, dtype=jnp.int32))
    return blocks.reshape(seq_total, HEADS * HEAD_DIM)

def reference(queries, keys_values, sink_logits, out_weight, expert_tokens, norm_gain, routes, route_weights, gate_weight, up_weight, down_weight):
    attended = attend_all(queries, keys_values, sink_logits)
    mixer_out = jnp.dot(attended, out_weight, preferred_element_type=jnp.float32).astype(jnp.bfloat16)
    token_total = expert_tokens.shape[0]
    block_count = token_total // MOE_ROWS
    rows_float = expert_tokens.astype(jnp.float32)
    centred = rows_float - lax.optimization_barrier(jnp.mean(rows_float, -1, keepdims=True))
    normed = (centred * lax.rsqrt(lax.optimization_barrier(jnp.mean(centred * centred, -1, keepdims=True)) + 1e-06) * norm_gain).astype(jnp.bfloat16)
    flat_routes = routes.reshape(block_count, MOE_ROWS * TOPK).astype(jnp.int32)
    one_hot = (flat_routes[:, :, None] == jnp.arange(EXPERTS, dtype=jnp.int32)[None, None, :]).astype(jnp.int32)
    slot_rank = lax.optimization_barrier(jnp.sum((jnp.cumsum(one_hot, 1) - 1) * one_hot, -1))
    block_ids = jnp.arange(block_count, dtype=jnp.int32)[:, None]
    expert_slot = (flat_routes * (block_count * CAP) + block_ids * CAP + slot_rank).reshape(-1)
    copy_token = (block_ids * MOE_ROWS + jnp.arange(MOE_ROWS * TOPK, dtype=jnp.int32)[None, :] // TOPK).reshape(-1)
    slot_table = jnp.full((EXPERTS * block_count * CAP,), token_total, jnp.int32).at[expert_slot].set(copy_token)
    slot_table = slot_table.reshape(EXPERTS, block_count * CAP)
    weight_table = jnp.zeros((EXPERTS * block_count * CAP,), jnp.float32).at[expert_slot].set(route_weights.reshape(-1))
    weight_table = weight_table.reshape(EXPERTS, block_count * CAP)
    quarter = FE // N_TP

    def add_expert(running, expert_index):
        token_index = slot_table[expert_index]
        chosen = jnp.take(normed, token_index, axis=0, mode='fill', fill_value=0)
        gate_value = jnp.dot(chosen, gate_weight[expert_index], preferred_element_type=jnp.float32)
        up_value = jnp.dot(chosen, up_weight[expert_index], preferred_element_type=jnp.float32)
        hidden = (jax.nn.silu(gate_value) * up_value).astype(jnp.bfloat16)
        hidden_parts = hidden.astype(jnp.float32).reshape(-1, N_TP, quarter)
        down_parts = down_weight[expert_index].astype(jnp.float32).reshape(N_TP, quarter, -1)
        partial_value = jnp.einsum('rqf,qfd->qrd', hidden_parts, down_parts)
        partial_value = lax.optimization_barrier(partial_value.astype(jnp.bfloat16)).astype(jnp.float32)
        copy_result = lax.optimization_barrier(jnp.sum(partial_value, 0)).astype(jnp.bfloat16)
        update = lax.optimization_barrier(copy_result).astype(jnp.float32) * weight_table[expert_index][:, None]
        return (running.at[token_index].add(update, mode='drop'), None)
    total_out, unused = lax.scan(add_expert, jnp.zeros((token_total, expert_tokens.shape[1]), jnp.float32), jnp.arange(EXPERTS, dtype=jnp.int32))
    expert_out = total_out.astype(jnp.bfloat16)
    return (mixer_out, expert_out)
```

```python
import functools

import jax
import jax.numpy as jnp
from jax import lax
from jax.experimental import pallas as pl
from jax.experimental.pallas import tpu as pltpu
from jax.sharding import PartitionSpec as P

MESH = pl.DeviceIdType.MESH
HEAD_DIM = 64
WINDOW = 128
CAP = 24
F32 = jnp.float32
BF16 = jnp.bfloat16
NEG_FILL = -1e30

GU_CHUNKS = 4
DOWN_CHUNKS = 4


def kernel(
    n_ep,
    n_tp,
    q_hbm,
    kv_hbm,
    sink_ref,
    ow_hbm,
    tok_hbm,
    gain_ref,
    routes_ref,
    rw_ref,
    g_hbm,
    u_hbm,
    d_hbm,
    mix_hbm,
    exp_hbm,
    q_v,
    kv_v,
    ow_v,
    tok_v,
    normed_v,
    slots_v,
    comb_v,
    out_v,
    arr_v,
    gu_v,
    down_v,
    hid_v,
    back_v,
    ret_v,
    att_v,
    attin_v,
    mix_v,
    eout_v,
    loc_sem,
    halo_ssem,
    halo_rsem,
    gu_ssem,
    gu_rsem,
    gur_ssem,
    gur_rsem,
    dn_ssem,
    dn_rsem,
    dnr_ssem,
    dnr_rsem,
    disp_sem,
    ret_ssem,
    ret_rsem,
    att_sem,
    fin_sem,
):
    ep = lax.axis_index("ep")
    tp = lax.axis_index("tp")
    right = lax.rem(tp + 1, n_tp)
    left = lax.rem(tp + n_tp - 1, n_tp)
    next_ep = lax.rem(ep + 1, n_ep)
    prev_ep = lax.rem(ep + n_ep - 1, n_ep)
    rows = q_v.shape[0]
    width = tok_v.shape[1]
    half = width // 2
    hid = gu_v.shape[3]
    dcol = width // DOWN_CHUNKS
    slot_rows = n_ep * CAP

    def local(src, dst, k):
        return pltpu.make_async_copy(src, dst, loc_sem.at[k])

    loads = [
        local(tok_hbm, tok_v, 0),
        local(q_hbm, q_v, 1),
        local(kv_hbm, kv_v.at[pl.ds(WINDOW, rows)], 2),
        local(g_hbm.at[0], gu_v.at[0, 0], 3),
        local(u_hbm.at[0], gu_v.at[0, 1], 4),
        local(ow_hbm, ow_v, 5),
    ]
    for c in range(DOWN_CHUNKS):
        loads.append(local(d_hbm.at[0, :, pl.ds(c * dcol, dcol)], down_v.at[c, pl.ds(0, hid)], 6 + c))
    for copy in loads:
        copy.start()

    barrier = pltpu.get_barrier_semaphore()

    @pl.loop(1, n_ep)
    def _(d):
        pl.semaphore_signal(
            barrier, inc=1, device_id=(lax.rem(ep + d, n_ep), tp), device_id_type=MESH
        )

    for j in range(1, n_tp):
        pl.semaphore_signal(
            barrier, inc=1, device_id=(ep, lax.rem(tp + j, n_tp)), device_id_type=MESH
        )
    pl.semaphore_wait(barrier, n_ep - 1 + n_tp - 1)

    def remote(src, dst, ssem, rsem, device):
        return pltpu.make_async_remote_copy(
            src_ref=src,
            dst_ref=dst,
            send_sem=ssem,
            recv_sem=rsem,
            device_id=device,
            device_id_type=MESH,
        )

    halos = [
        remote(
            kv_hbm.at[pl.ds(rows - WINDOW, WINDOW)],
            kv_v.at[pl.ds(0, WINDOW)],
            halo_ssem.at[0],
            halo_rsem.at[0],
            (next_ep, tp),
        ),
        remote(
            kv_hbm.at[pl.ds(0, WINDOW)],
            kv_v.at[pl.ds(WINDOW + rows, WINDOW)],
            halo_ssem.at[1],
            halo_rsem.at[1],
            (prev_ep, tp),
        ),
    ]
    for copy in halos:
        copy.start()

    def gu_own(side, k):
        which = k % 2
        part = (k // 2 + side) % 2
        src = (g_hbm, u_hbm)[which].at[0, pl.ds(part * half, half)]
        dst = gu_v.at[1 + side, which, pl.ds(part * half, half)]
        return remote(
            src, dst, gu_ssem.at[side, k], gu_rsem.at[side, k], (ep, (right, left)[side])
        )

    def gu_relay(side, k):
        src = gu_v.at[1 + side, k, pl.ds(side * half, half)]
        dst = gu_v.at[3, k, pl.ds(side * half, half)]
        return remote(
            src, dst, gur_ssem.at[side, k], gur_rsem.at[side, k], (ep, (right, left)[side])
        )

    def dn_own(side, c):
        src = d_hbm.at[0, :, pl.ds(c * dcol, dcol)]
        dst = down_v.at[c, pl.ds((1 + side) * hid, hid)]
        return remote(
            src, dst, dn_ssem.at[side, c], dn_rsem.at[side, c], (ep, (right, left)[side])
        )

    def dn_relay(side, c):
        at = side * (hid // 2)
        src = down_v.at[c, pl.ds((1 + side) * hid + at, hid // 2)]
        dst = down_v.at[c, pl.ds(3 * hid + at, hid // 2)]
        return remote(
            src, dst, dnr_ssem.at[side, c], dnr_rsem.at[side, c], (ep, (right, left)[side])
        )

    for k in range(GU_CHUNKS):
        for side in range(2):
            gu_own(side, k).start()

    loads[0].wait()

    @pl.loop(0, 8)
    def _(i):
        at = pl.ds(pl.multiple_of(i * 32, 32), 32)
        x = tok_v[at, :].astype(F32)
        x = x - jnp.mean(x, -1, keepdims=True)
        var = jnp.mean(x * x, -1, keepdims=True)
        normed_v[at, :] = (x * lax.rsqrt(var + 1e-06) * gain_ref[...]).astype(BF16)

    tokens = tok_v.shape[0]
    first = routes_ref[0:1, :]
    second = routes_ref[1:2, :]
    expert_ids = lax.broadcasted_iota(jnp.int32, (n_ep, tokens), 0)
    is_first = expert_ids == first
    is_second = expert_ids == second
    named = is_first | is_second
    before = (
        lax.broadcasted_iota(jnp.int32, (tokens, tokens), 0)
        < lax.broadcasted_iota(jnp.int32, (tokens, tokens), 1)
    ).astype(F32)
    named_f = named.astype(F32)
    rank = jnp.dot(named_f.astype(BF16), before.astype(BF16), preferred_element_type=F32)
    rank = jnp.where(named, rank, -1.0).astype(BF16)
    weight = jnp.where(is_first, rw_ref[0:1, :], 0.0) + jnp.where(is_second, rw_ref[1:2, :], 0.0)
    weight_hi = weight.astype(BF16)
    weight_lo = (weight - weight_hi.astype(F32)).astype(BF16)

    def slot_expert(shape, axis):
        slot = lax.broadcasted_iota(jnp.int32, shape, axis).astype(F32)
        expert = jnp.floor((slot + 0.5) * (1.0 / CAP))
        return expert, slot - expert * CAP

    expert, place = slot_expert((slot_rows, n_ep), 0)
    spread = (expert == lax.broadcasted_iota(jnp.int32, (slot_rows, n_ep), 1).astype(F32)).astype(
        F32
    )
    _, place_t = slot_expert((slot_rows, tokens), 0)
    ranks = jnp.dot(spread.astype(BF16), rank, preferred_element_type=F32)
    slots_v[...] = jnp.where(ranks == place_t, 1.0, 0.0).astype(BF16)

    per_block = 8 * CAP

    @pl.loop(0, slot_rows // per_block)
    def _(i):
        at = pl.ds(pl.multiple_of(i * per_block, per_block), per_block)
        picked = jnp.dot(slots_v[at, :], normed_v[...], preferred_element_type=F32)
        out_v[pl.ds(i * 8, 8)] = picked.astype(BF16).reshape(8, CAP, width)

    @pl.loop(1, n_ep)
    def _(d):
        to = lax.rem(ep + d, n_ep)
        remote(out_v.at[to], arr_v.at[ep], disp_sem.at[0], disp_sem.at[1], (to, tp)).start()

    arr_v[ep] = out_v[ep]

    expert_c = jnp.floor((lax.broadcasted_iota(jnp.int32, (n_ep, slot_rows), 1).astype(F32) + 0.5) * (1.0 / CAP))
    spread_t = (
        expert_c == lax.broadcasted_iota(jnp.int32, (n_ep, slot_rows), 0).astype(F32)
    ).astype(F32).astype(BF16)

    def over_slots(table):
        return lax.dot_general(
            table.astype(F32).T.astype(BF16),
            spread_t,
            (((1,), (0,)), ((), ())),
            preferred_element_type=F32,
        )

    _, place_c = slot_expert((tokens, slot_rows), 1)
    chosen = over_slots(rank) == place_c
    comb_v[0] = jnp.where(chosen, over_slots(weight_hi), 0.0).astype(BF16)
    comb_v[1] = jnp.where(chosen, over_slots(weight_lo), 0.0).astype(BF16)

    loads[1].wait()
    loads[2].wait()
    for copy in halos:
        copy.wait_recv()
    block = 128
    span = block + 2 * WINDOW
    heads = q_v.shape[1] // HEAD_DIM
    blocks_per_dest = rows // block // n_tp
    rel = lax.broadcasted_iota(jnp.int32, (block, span), 1) - lax.broadcasted_iota(
        jnp.int32, (block, span), 0
    )
    key_at = lax.broadcasted_iota(jnp.int32, (block, span), 1)
    seq_total = rows * n_ep

    @pl.loop(0, rows // block)
    def _(b):
        row = pl.multiple_of(b * block, block)
        q = q_v[pl.ds(row, block), :] * jnp.asarray(HEAD_DIM**-0.5, BF16)
        kv = kv_v[pl.ds(row, span), :]
        keys = kv[:, 0:HEAD_DIM]
        values = kv[:, HEAD_DIM : 2 * HEAD_DIM]
        key_pos = key_at + (ep * rows + row - WINDOW)
        allowed = (rel >= 0) & (rel <= 2 * WINDOW) & (key_pos >= 0) & (key_pos < seq_total)
        outs = []
        for h in range(heads):
            sink = sink_ref[tp * heads + h]
            scores = lax.dot_general(
                q[:, h * HEAD_DIM : (h + 1) * HEAD_DIM],
                keys,
                (((1,), (1,)), ((), ())),
                preferred_element_type=F32,
            )
            scores = jnp.where(allowed, scores, NEG_FILL)
            top = jnp.maximum(jnp.max(scores, -1, keepdims=True), sink)
            expo = jnp.exp(scores - top)
            denom = jnp.sum(expo, -1, keepdims=True) + jnp.exp(sink - top)
            mixed = jnp.dot(expo.astype(BF16), values, preferred_element_type=F32)
            outs.append((mixed / denom).astype(BF16))
        att_v[b // blocks_per_dest, pl.ds(pl.multiple_of(lax.rem(b, blocks_per_dest) * block, block), block), :] = (
            jnp.concatenate(outs, axis=1)
        )

    attin_v[tp] = att_v[tp]

    for k in range(2):
        for side in range(2):
            gu_own(side, k).wait_recv()
            gu_relay(side, k).start()
    for c in range(2):
        for side in range(2):
            dn_own(side, c).start()

    arrived = arr_v.at[pl.ds(0, n_ep - 1)]
    pltpu.make_async_copy(arrived, arrived, disp_sem.at[1]).wait()

    def widen(s):
        @pl.loop(0, slot_rows // per_block)
        def _(i):
            x = arr_v[pl.ds(i * 8, 8)].reshape(per_block, width)
            g = jnp.dot(x, gu_v[s, 0], preferred_element_type=F32)
            u = jnp.dot(x, gu_v[s, 1], preferred_element_type=F32)
            at = pl.ds(pl.multiple_of(i * per_block, per_block), per_block)
            hid_v[s, at, :] = (g / (1.0 + jnp.exp(-g)) * u).astype(BF16)

    loads[3].wait()
    loads[4].wait()
    widen(0)
    for k in range(2, GU_CHUNKS):
        for side in range(2):
            gu_own(side, k).wait_recv()

    @pl.loop(1, 3)
    def _(s):
        widen(s)

    for k in range(2):
        for side in range(2):
            gu_relay(side, k).wait_recv()
    widen(3)

    for c in range(DOWN_CHUNKS):
        for side in range(2):
            dn_own(side, c).wait_recv()
            dn_relay(side, c).start()
        if c + 2 < DOWN_CHUNKS:
            for side in range(2):
                dn_own(side, c + 2).start()
        if c == DOWN_CHUNKS - 1:
            for j in range(1, n_tp):
                to = lax.rem(tp + j, n_tp)
                remote(
                    att_v.at[to], attin_v.at[tp], att_sem.at[0], att_sem.at[1], (ep, to)
                ).start()
        loads[6 + c].wait()
        for side in range(2):
            dn_relay(side, c).wait_recv()

        @pl.loop(0, slot_rows // per_block)
        def _(i):
            at = pl.ds(pl.multiple_of(i * per_block, per_block), per_block)
            total = jnp.zeros((per_block, dcol), F32)
            for s in range(4):
                total = total + jnp.dot(
                    hid_v[s, at, :],
                    down_v[c, s * hid : (s + 1) * hid, :],
                    preferred_element_type=F32,
                )
            back_v[c, pl.ds(i * 8, 8)] = total.astype(BF16).reshape(8, CAP, dcol)

        @pl.loop(1, n_ep)
        def _(d):
            to = lax.rem(ep + d, n_ep)
            remote(
                back_v.at[c, to], ret_v.at[c, ep], ret_ssem.at[c], ret_rsem.at[c], (to, tp)
            ).start()

        ret_v[c, ep] = back_v[c, ep]

    def combine(c):
        got = ret_v.at[c, pl.ds(0, n_ep - 1)]
        pltpu.make_async_copy(got, got, ret_rsem.at[c]).wait()
        results = ret_v[c].reshape(slot_rows, dcol)
        total = jnp.dot(comb_v[0], results, preferred_element_type=F32) + jnp.dot(
            comb_v[1], results, preferred_element_type=F32
        )
        eout_v[c] = total.astype(BF16)
        pltpu.make_async_copy(
            eout_v.at[c], exp_hbm.at[:, pl.ds(c * dcol, dcol)], fin_sem.at[c]
        ).start()

    combine(0)
    combine(1)

    loads[5].wait()
    got = attin_v.at[pl.ds(0, n_tp - 1)]
    pltpu.make_async_copy(got, got, att_sem.at[1]).wait()
    mcol = mix_v.shape[2]
    head_cols = heads * HEAD_DIM

    def mix_out(c):
        return pltpu.make_async_copy(
            mix_v.at[c], mix_hbm.at[:, pl.ds(c * mcol, mcol)], fin_sem.at[DOWN_CHUNKS + c]
        )

    for c in range(mix_v.shape[0]):
        total = jnp.zeros((mix_v.shape[1], mcol), F32)
        for s in range(n_tp):
            total = total + jnp.dot(
                attin_v[s],
                ow_v[s * head_cols : (s + 1) * head_cols, c * mcol : (c + 1) * mcol],
                preferred_element_type=F32,
            )
        mix_v[c] = total.astype(BF16)
        mix_out(c).start()

    combine(2)
    combine(3)

    for c in range(DOWN_CHUNKS):
        pltpu.make_async_copy(
            eout_v.at[c], exp_hbm.at[:, pl.ds(c * dcol, dcol)], fin_sem.at[c]
        ).wait()
    for c in range(mix_v.shape[0]):
        mix_out(c).wait()
    for copy in halos:
        copy.wait_send()
    for side in range(2):
        for k in range(GU_CHUNKS):
            gu_own(side, k).wait_send()
        for k in range(2):
            gu_relay(side, k).wait_send()
        for c in range(DOWN_CHUNKS):
            dn_own(side, c).wait_send()
            dn_relay(side, c).wait_send()
    sent = out_v.at[pl.ds(0, n_ep - 1)]
    pltpu.make_async_copy(sent, sent, disp_sem.at[0]).wait()
    for c in range(DOWN_CHUNKS):
        sent = back_v.at[c, pl.ds(0, n_ep - 1)]
        pltpu.make_async_copy(sent, sent, ret_ssem.at[c]).wait()
    sent = att_v.at[pl.ds(0, n_tp - 1)]
    pltpu.make_async_copy(sent, sent, att_sem.at[0]).wait()


def body(
    queries,
    keys_values,
    sink_logits,
    out_weight,
    expert_tokens,
    norm_gain,
    routes,
    route_weights,
    gate_weight,
    up_weight,
    down_weight,
):
    n_ep = lax.axis_size("ep")
    n_tp = lax.axis_size("tp")
    rows, q_cols = queries.shape
    tokens, width = expert_tokens.shape
    hid = gate_weight.shape[2]
    out_rows = rows // n_tp
    dcol = width // DOWN_CHUNKS
    mcol = width // 4
    slot_rows = n_ep * CAP
    any_space = pl.BlockSpec(memory_space=pl.ANY)
    vmem = pl.BlockSpec(memory_space=pltpu.VMEM)
    smem = pl.BlockSpec(memory_space=pltpu.SMEM)
    dma = pltpu.SemaphoreType.DMA
    return pl.pallas_call(
        functools.partial(kernel, n_ep, n_tp),
        out_shape=(
            jax.ShapeDtypeStruct((out_rows, width), BF16),
            jax.ShapeDtypeStruct((tokens, width), BF16),
        ),
        in_specs=[
            any_space,
            any_space,
            smem,
            any_space,
            any_space,
            vmem,
            vmem,
            vmem,
            any_space,
            any_space,
            any_space,
        ],
        out_specs=(any_space, any_space),
        scratch_shapes=[
            pltpu.VMEM((rows, q_cols), BF16),
            pltpu.VMEM((rows + 2 * WINDOW, 2 * HEAD_DIM), BF16),
            pltpu.VMEM(out_weight.shape, BF16),
            pltpu.VMEM((tokens, width), BF16),
            pltpu.VMEM((tokens, width), BF16),
            pltpu.VMEM((slot_rows, tokens), BF16),
            pltpu.VMEM((2, tokens, slot_rows), BF16),
            pltpu.VMEM((n_ep, CAP, width), BF16),
            pltpu.VMEM((n_ep, CAP, width), BF16),
            pltpu.VMEM((4, 2, width, hid), BF16),
            pltpu.VMEM((DOWN_CHUNKS, 4 * hid, dcol), BF16),
            pltpu.VMEM((4, slot_rows, hid), BF16),
            pltpu.VMEM((DOWN_CHUNKS, n_ep, CAP, dcol), BF16),
            pltpu.VMEM((DOWN_CHUNKS, n_ep, CAP, dcol), BF16),
            pltpu.VMEM((n_tp, out_rows, q_cols), BF16),
            pltpu.VMEM((n_tp, out_rows, q_cols), BF16),
            pltpu.VMEM((4, out_rows, mcol), BF16),
            pltpu.VMEM((DOWN_CHUNKS, tokens, dcol), BF16),
            dma((6 + DOWN_CHUNKS,)),
            dma((2,)),
            dma((2,)),
            dma((2, GU_CHUNKS)),
            dma((2, GU_CHUNKS)),
            dma((2, 2)),
            dma((2, 2)),
            dma((2, DOWN_CHUNKS)),
            dma((2, DOWN_CHUNKS)),
            dma((2, DOWN_CHUNKS)),
            dma((2, DOWN_CHUNKS)),
            dma((2,)),
            dma((DOWN_CHUNKS,)),
            dma((DOWN_CHUNKS,)),
            dma((2,)),
            dma((DOWN_CHUNKS + 4,)),
        ],
        compiler_params=pltpu.CompilerParams(
            collective_id=0, has_side_effects=True, vmem_limit_bytes=60 * 1024 * 1024
        ),
    )(
        queries,
        keys_values,
        sink_logits,
        out_weight,
        expert_tokens,
        norm_gain.reshape(1, width),
        routes.T,
        route_weights.T,
        gate_weight,
        up_weight,
        down_weight,
    )


def solution(mesh):
    in_specs = (
        P("ep", "tp"),
        P("ep", "tp"),
        P(),
        P(),
        P(("ep", "tp"), None),
        P(),
        P(("ep", "tp"), None),
        P(("ep", "tp"), None),
        P("ep", None, "tp"),
        P("ep", None, "tp"),
        P("ep", "tp", None),
    )
    out_specs = (P(("ep", "tp"), None), P(("ep", "tp"), None))
    return jax.shard_map(body, mesh=mesh, in_specs=in_specs, out_specs=out_specs, check_vma=False)
```

```python
import functools

import jax
import jax.numpy as jnp
from jax import lax
from jax.experimental import pallas as pl
from jax.experimental.pallas import tpu as pltpu
from jax.sharding import PartitionSpec as P

MESH = pl.DeviceIdType.MESH
HEAD_DIM = 64
WINDOW = 128
CAP = 24
F32 = jnp.float32
BF16 = jnp.bfloat16
NEG_FILL = -1e30

GU_CHUNKS = 4
DOWN_CHUNKS = 8
ATT_PARTS = 4


def kernel(
    n_ep,
    n_tp,
    q_hbm,
    kv_hbm,
    sink_hbm,
    ow_hbm,
    tok_hbm,
    gain_hbm,
    routes_hbm,
    rw_hbm,
    g_hbm,
    u_hbm,
    d_hbm,
    mix_ref,
    exp_ref,
    sink_ref,
    gain_ref,
    routes_ref,
    rw_ref,
    q_v,
    kv_v,
    ow_v,
    tok_v,
    normed_v,
    slots_v,
    comb_v,
    out_v,
    arr_v,
    gu_v,
    down_v,
    hid_v,
    back_v,
    ret_v,
    att_v,
    attin_v,
    pass_v,
    loc_sem,
    halo_ssem,
    halo_rsem,
    gu_ssem,
    gu_rsem,
    gur_ssem,
    gur_rsem,
    dn_ssem,
    dn_rsem,
    dnr_ssem,
    dnr_rsem,
    disp_sem,
    ret_ssem,
    ret_rsem,
    far_ssem,
    far_rsem,
    fwd_ssem,
    fwd_rsem,
    att_ssem,
    att_rsem,
):
    ep = lax.axis_index("ep")
    tp = lax.axis_index("tp")
    right = lax.rem(tp + 1, n_tp)
    left = lax.rem(tp + n_tp - 1, n_tp)
    next_ep = lax.rem(ep + 1, n_ep)
    prev_ep = lax.rem(ep + n_ep - 1, n_ep)
    rows = q_v.shape[0]
    width = tok_v.shape[1]
    half = width // 2
    hid = gu_v.shape[3]
    dcol = width // DOWN_CHUNKS
    slot_rows = n_ep * CAP

    def local(src, dst, k):
        return pltpu.make_async_copy(src, dst, loc_sem.at[k])

    loads = [
        local(tok_hbm, tok_v, 0),
        local(q_hbm, q_v, 1),
        local(kv_hbm, kv_v.at[pl.ds(WINDOW, rows)], 2),
        local(g_hbm.at[0], gu_v.at[0, 0], 3),
        local(u_hbm.at[0], gu_v.at[0, 1], 4),
        local(ow_hbm, ow_v, 5),
        local(gain_hbm, gain_ref, 6),
        local(routes_hbm, routes_ref, 7),
        local(rw_hbm, rw_ref, 8),
        local(sink_hbm, sink_ref, 9),
    ]
    for c in range(DOWN_CHUNKS):
        loads.append(local(d_hbm.at[0, :, pl.ds(c * dcol, dcol)], down_v.at[c, pl.ds(0, hid)], 10 + c))
    barrier = pltpu.get_barrier_semaphore()

    def greet(semaphore, device):
        pl.semaphore_signal(semaphore, inc=1, device_id=device, device_id_type=MESH)

    greet(barrier, (ep, right))
    greet(barrier, (ep, left))

    @pl.loop(1, n_ep)
    def _(d):
        greet(barrier, (lax.rem(ep + d, n_ep), tp))

    pl.semaphore_wait(barrier, 2 + n_ep - 1)

    def remote(src, dst, ssem, rsem, device):
        return pltpu.make_async_remote_copy(
            src_ref=src,
            dst_ref=dst,
            send_sem=ssem,
            recv_sem=rsem,
            device_id=device,
            device_id_type=MESH,
        )

    halos = [
        remote(
            kv_hbm.at[pl.ds(rows - WINDOW, WINDOW)],
            kv_v.at[pl.ds(0, WINDOW)],
            halo_ssem.at[0],
            halo_rsem.at[0],
            (next_ep, tp),
        ),
        remote(
            kv_hbm.at[pl.ds(0, WINDOW)],
            kv_v.at[pl.ds(WINDOW + rows, WINDOW)],
            halo_ssem.at[1],
            halo_rsem.at[1],
            (prev_ep, tp),
        ),
    ]
    def gu_own(side, k):
        which = k % 2
        part = (k // 2 + side) % 2
        src = (g_hbm, u_hbm)[which].at[0, pl.ds(part * half, half)]
        dst = gu_v.at[1 + side, which, pl.ds(part * half, half)]
        return remote(
            src, dst, gu_ssem.at[side, k], gu_rsem.at[side, k], (ep, (right, left)[side])
        )

    def gu_relay(side, k):
        src = gu_v.at[1 + side, k, pl.ds(side * half, half)]
        dst = gu_v.at[3, k, pl.ds(side * half, half)]
        return remote(
            src, dst, gur_ssem.at[side, k], gur_rsem.at[side, k], (ep, (right, left)[side])
        )

    def dn_own(side, c):
        src = d_hbm.at[0, :, pl.ds(c * dcol, dcol)]
        dst = down_v.at[c, pl.ds((1 + side) * hid, hid)]
        return remote(
            src, dst, dn_ssem.at[side, c], dn_rsem.at[side, c], (ep, (right, left)[side])
        )

    def dn_relay(side, c):
        at = side * (hid // 2)
        src = down_v.at[c, pl.ds((1 + side) * hid + at, hid // 2)]
        dst = down_v.at[c, pl.ds(3 * hid + at, hid // 2)]
        return remote(
            src, dst, dnr_ssem.at[side, c], dnr_rsem.at[side, c], (ep, (right, left)[side])
        )

    opposite = lax.rem(tp + 2, n_tp)
    part_rows = att_v.shape[1] // ATT_PARTS
    part_cols = att_v.shape[2] // 2

    def att_far(side, p):
        at = pl.ds(p * part_rows, part_rows)
        src = att_v.at[opposite, at, pl.ds(side * part_cols, part_cols)]
        dst = pass_v.at[side, p]
        return remote(
            src, dst, far_ssem.at[side, p], far_rsem.at[side, p], (ep, (right, left)[side])
        )

    def att_fwd(side, p):
        at = pl.ds(p * part_rows, part_rows)
        dst = attin_v.at[(left, right)[side], at, pl.ds(side * part_cols, part_cols)]
        return remote(
            pass_v.at[side, p],
            dst,
            fwd_ssem.at[side, p],
            fwd_rsem.at[side, p],
            (ep, (right, left)[side]),
        )

    def att_near(side, p):
        at = pl.ds(p * part_rows, part_rows)
        to = (right, left)[side]
        return remote(
            att_v.at[to, at], attin_v.at[tp, at], att_ssem.at[side, p], att_rsem.at[side, p], (ep, to)
        )

    for k in range(GU_CHUNKS):
        for side in range(2):
            gu_own(side, k).start()

    for copy in loads:
        copy.start()

    loads[0].wait()
    for k in range(6, 10):
        loads[k].wait()

    @pl.loop(0, 8)
    def _(i):
        at = pl.ds(pl.multiple_of(i * 32, 32), 32)
        x = tok_v[at, :].astype(F32)
        x = x - jnp.mean(x, -1, keepdims=True)
        var = jnp.mean(x * x, -1, keepdims=True)
        normed_v[at, :] = (x * lax.rsqrt(var + 1e-06) * gain_ref[...]).astype(BF16)

    tokens = tok_v.shape[0]
    first = routes_ref[0:1, :]
    second = routes_ref[1:2, :]
    expert_ids = lax.broadcasted_iota(jnp.int32, (n_ep, tokens), 0)
    is_first = expert_ids == first
    is_second = expert_ids == second
    named = is_first | is_second
    before = (
        lax.broadcasted_iota(jnp.int32, (tokens, tokens), 0)
        < lax.broadcasted_iota(jnp.int32, (tokens, tokens), 1)
    ).astype(F32)
    named_f = named.astype(F32)
    rank = jnp.dot(named_f.astype(BF16), before.astype(BF16), preferred_element_type=F32)
    rank = jnp.where(named, rank, -1.0).astype(BF16)
    weight = jnp.where(is_first, rw_ref[0:1, :], 0.0) + jnp.where(is_second, rw_ref[1:2, :], 0.0)
    weight_hi = weight.astype(BF16)
    weight_lo = (weight - weight_hi.astype(F32)).astype(BF16)

    def slot_expert(shape, axis):
        slot = lax.broadcasted_iota(jnp.int32, shape, axis).astype(F32)
        expert = jnp.floor((slot + 0.5) * (1.0 / CAP))
        return expert, slot - expert * CAP

    expert, place = slot_expert((slot_rows, n_ep), 0)
    spread = (expert == lax.broadcasted_iota(jnp.int32, (slot_rows, n_ep), 1).astype(F32)).astype(
        F32
    )
    _, place_t = slot_expert((slot_rows, tokens), 0)
    ranks = jnp.dot(spread.astype(BF16), rank, preferred_element_type=F32)
    slots_v[...] = jnp.where(ranks == place_t, 1.0, 0.0).astype(BF16)

    per_block = 8 * CAP

    @pl.loop(0, slot_rows // per_block)
    def _(i):
        at = pl.ds(pl.multiple_of(i * per_block, per_block), per_block)
        picked = jnp.dot(slots_v[at, :], normed_v[...], preferred_element_type=F32)
        out_v[pl.ds(i * 8, 8)] = picked.astype(BF16).reshape(8, CAP, width)

    expert_c = jnp.floor((lax.broadcasted_iota(jnp.int32, (n_ep, slot_rows), 1).astype(F32) + 0.5) * (1.0 / CAP))
    spread_t = (
        expert_c == lax.broadcasted_iota(jnp.int32, (n_ep, slot_rows), 0).astype(F32)
    ).astype(F32).astype(BF16)

    def over_slots(table):
        return lax.dot_general(
            table.astype(F32).T.astype(BF16),
            spread_t,
            (((1,), (0,)), ((), ())),
            preferred_element_type=F32,
        )

    _, place_c = slot_expert((tokens, slot_rows), 1)
    chosen = over_slots(rank) == place_c
    comb_v[0] = jnp.where(chosen, over_slots(weight_hi), 0.0).astype(BF16)
    comb_v[1] = jnp.where(chosen, over_slots(weight_lo), 0.0).astype(BF16)

    for copy in halos:
        copy.start()

    @pl.loop(1, n_ep)
    def _(d):
        to = lax.rem(ep + d, n_ep)
        remote(out_v.at[to], arr_v.at[ep], disp_sem.at[0], disp_sem.at[1], (to, tp)).start()

    arr_v[ep] = out_v[ep]

    loads[1].wait()
    loads[2].wait()
    for copy in halos:
        copy.wait_recv()
    block = 128
    span = block + 2 * WINDOW
    heads = q_v.shape[1] // HEAD_DIM
    blocks_per_dest = rows // block // n_tp
    rel = lax.broadcasted_iota(jnp.int32, (block, span), 1) - lax.broadcasted_iota(
        jnp.int32, (block, span), 0
    )
    key_at = lax.broadcasted_iota(jnp.int32, (block, span), 1)
    seq_total = rows * n_ep

    @pl.loop(0, rows // block)
    def _(b):
        row = pl.multiple_of(b * block, block)
        q = q_v[pl.ds(row, block), :] * jnp.asarray(HEAD_DIM**-0.5, BF16)
        kv = kv_v[pl.ds(row, span), :]
        keys = kv[:, 0:HEAD_DIM]
        values = kv[:, HEAD_DIM : 2 * HEAD_DIM]
        key_pos = key_at + (ep * rows + row - WINDOW)
        allowed = (rel >= 0) & (rel <= 2 * WINDOW) & (key_pos >= 0) & (key_pos < seq_total)
        outs = []
        for h in range(heads):
            sink = sink_ref[tp * heads + h]
            scores = lax.dot_general(
                q[:, h * HEAD_DIM : (h + 1) * HEAD_DIM],
                keys,
                (((1,), (1,)), ((), ())),
                preferred_element_type=F32,
            )
            scores = jnp.where(allowed, scores, NEG_FILL)
            top = jnp.maximum(jnp.max(scores, -1, keepdims=True), sink)
            expo = jnp.exp(scores - top)
            denom = jnp.sum(expo, -1, keepdims=True) + jnp.exp(sink - top)
            mixed = jnp.dot(expo.astype(BF16), values, preferred_element_type=F32)
            outs.append((mixed / denom).astype(BF16))
        att_v[b // blocks_per_dest, pl.ds(pl.multiple_of(lax.rem(b, blocks_per_dest) * block, block), block), :] = (
            jnp.concatenate(outs, axis=1)
        )

    attin_v[tp] = att_v[tp]

    for k in range(2):
        for side in range(2):
            gu_own(side, k).wait_recv()
            gu_relay(side, k).start()
    for c in range(2):
        for side in range(2):
            dn_own(side, c).start()

    arrived = arr_v.at[pl.ds(0, n_ep - 1)]
    pltpu.make_async_copy(arrived, arrived, disp_sem.at[1]).wait()

    def widen(s):
        @pl.loop(0, slot_rows // per_block)
        def _(i):
            x = arr_v[pl.ds(i * 8, 8)].reshape(per_block, width)
            g = jnp.dot(x, gu_v[s, 0], preferred_element_type=F32)
            u = jnp.dot(x, gu_v[s, 1], preferred_element_type=F32)
            at = pl.ds(pl.multiple_of(i * per_block, per_block), per_block)
            hid_v[s, at, :] = (g / (1.0 + jnp.exp(-g)) * u).astype(BF16)

    loads[3].wait()
    loads[4].wait()
    widen(0)
    for k in range(2, GU_CHUNKS):
        for side in range(2):
            gu_own(side, k).wait_recv()

    @pl.loop(1, 3)
    def _(s):
        widen(s)

    for k in range(2):
        for side in range(2):
            gu_relay(side, k).wait_recv()
    widen(3)

    def combine(c):
        got = ret_v.at[c, pl.ds(0, n_ep - 1)]
        pltpu.make_async_copy(got, got, ret_rsem.at[c]).wait()
        results = ret_v[c].reshape(slot_rows, dcol)
        total = jnp.dot(comb_v[0], results, preferred_element_type=F32) + jnp.dot(
            comb_v[1], results, preferred_element_type=F32
        )
        exp_ref[:, c * dcol : (c + 1) * dcol] = total.astype(BF16)

    def pass_on(c):
        for side in range(2):
            dn_own(side, c).wait_recv()
            dn_relay(side, c).start()
        if c + 2 < DOWN_CHUNKS:
            for side in range(2):
                dn_own(side, c + 2).start()
        if c + 1 == DOWN_CHUNKS:
            for send in (att_far, att_near):
                for p in range(ATT_PARTS):
                    for side in range(2):
                        send(side, p).start()

    pass_on(0)
    for c in range(DOWN_CHUNKS):
        loads[10 + c].wait()
        for side in range(2):
            dn_relay(side, c).wait_recv()
        if c + 1 < DOWN_CHUNKS:
            pass_on(c + 1)

        @pl.loop(0, slot_rows // per_block)
        def _(i):
            at = pl.ds(pl.multiple_of(i * per_block, per_block), per_block)
            total = jnp.zeros((per_block, dcol), F32)
            for s in range(4):
                total = total + jnp.dot(
                    hid_v[s, at, :],
                    down_v[c, s * hid : (s + 1) * hid, :],
                    preferred_element_type=F32,
                )
            back_v[c, pl.ds(i * 8, 8)] = total.astype(BF16).reshape(8, CAP, dcol)

        @pl.loop(1, n_ep)
        def _(d):
            to = lax.rem(ep + d, n_ep)
            remote(
                back_v.at[c, to], ret_v.at[c, ep], ret_ssem.at[c], ret_rsem.at[c], (to, tp)
            ).start()

        ret_v[c, ep] = back_v[c, ep]
        if 4 <= c < DOWN_CHUNKS - 1:
            combine(c - 4)

    for p in range(ATT_PARTS):
        for side in range(2):
            att_far(side, p).wait_recv()
            att_fwd(side, p).start()
    combine(DOWN_CHUNKS - 5)

    loads[5].wait()
    head_cols = heads * HEAD_DIM
    mcol = mix_ref.shape[1] // 4

    def project(p):
        for side in range(2):
            att_near(side, p).wait_recv()
            att_fwd(side, p).wait_recv()
        at = pl.ds(p * part_rows, part_rows)
        for n in range(4):
            total = jnp.zeros((part_rows, mcol), F32)
            for s in range(n_tp):
                total = total + jnp.dot(
                    attin_v[s, at, :],
                    ow_v[s * head_cols : (s + 1) * head_cols, n * mcol : (n + 1) * mcol],
                    preferred_element_type=F32,
                )
            mix_ref[at, n * mcol : (n + 1) * mcol] = total.astype(BF16)

    combine(DOWN_CHUNKS - 4)
    combine(DOWN_CHUNKS - 3)
    for p in range(ATT_PARTS - 1):
        project(p)
    combine(DOWN_CHUNKS - 2)
    project(ATT_PARTS - 1)
    combine(DOWN_CHUNKS - 1)

    for copy in halos:
        copy.wait_send()
    for side in range(2):
        for k in range(GU_CHUNKS):
            gu_own(side, k).wait_send()
        for k in range(2):
            gu_relay(side, k).wait_send()
        for c in range(DOWN_CHUNKS):
            dn_own(side, c).wait_send()
            dn_relay(side, c).wait_send()
        for p in range(ATT_PARTS):
            att_far(side, p).wait_send()
            att_fwd(side, p).wait_send()
            att_near(side, p).wait_send()
    sent = out_v.at[pl.ds(0, n_ep - 1)]
    pltpu.make_async_copy(sent, sent, disp_sem.at[0]).wait()
    for c in range(DOWN_CHUNKS):
        sent = back_v.at[c, pl.ds(0, n_ep - 1)]
        pltpu.make_async_copy(sent, sent, ret_ssem.at[c]).wait()


def body(
    queries,
    keys_values,
    sink_logits,
    out_weight,
    expert_tokens,
    norm_gain,
    routes,
    route_weights,
    gate_weight,
    up_weight,
    down_weight,
):
    n_ep = lax.axis_size("ep")
    n_tp = lax.axis_size("tp")
    rows, q_cols = queries.shape
    tokens, width = expert_tokens.shape
    hid = gate_weight.shape[2]
    out_rows = rows // n_tp
    dcol = width // DOWN_CHUNKS
    slot_rows = n_ep * CAP
    hbm = pl.BlockSpec(memory_space=pltpu.HBM)
    vmem = pl.BlockSpec(memory_space=pltpu.VMEM)
    dma = pltpu.SemaphoreType.DMA
    return pl.pallas_call(
        functools.partial(kernel, n_ep, n_tp),
        out_shape=(
            pltpu.VMEM((out_rows, width), BF16),
            pltpu.VMEM((tokens, width), BF16),
        ),
        in_specs=[hbm] * 11,
        out_specs=(vmem, vmem),
        scratch_shapes=[
            pltpu.SMEM(sink_logits.shape, F32),
            pltpu.VMEM((1, width), F32),
            pltpu.VMEM((2, tokens), jnp.int32),
            pltpu.VMEM((2, tokens), F32),
            pltpu.VMEM((rows, q_cols), BF16),
            pltpu.VMEM((rows + 2 * WINDOW, 2 * HEAD_DIM), BF16),
            pltpu.VMEM(out_weight.shape, BF16),
            pltpu.VMEM((tokens, width), BF16),
            pltpu.VMEM((tokens, width), BF16),
            pltpu.VMEM((slot_rows, tokens), BF16),
            pltpu.VMEM((2, tokens, slot_rows), BF16),
            pltpu.VMEM((n_ep, CAP, width), BF16),
            pltpu.VMEM((n_ep, CAP, width), BF16),
            pltpu.VMEM((4, 2, width, hid), BF16),
            pltpu.VMEM((DOWN_CHUNKS, 4 * hid, dcol), BF16),
            pltpu.VMEM((4, slot_rows, hid), BF16),
            pltpu.VMEM((DOWN_CHUNKS, n_ep, CAP, dcol), BF16),
            pltpu.VMEM((DOWN_CHUNKS, n_ep, CAP, dcol), BF16),
            pltpu.VMEM((n_tp, out_rows, q_cols), BF16),
            pltpu.VMEM((n_tp, out_rows, q_cols), BF16),
            pltpu.VMEM((2, ATT_PARTS, out_rows // ATT_PARTS, q_cols // 2), BF16),
            dma((10 + DOWN_CHUNKS,)),
            dma((2,)),
            dma((2,)),
            dma((2, GU_CHUNKS)),
            dma((2, GU_CHUNKS)),
            dma((2, 2)),
            dma((2, 2)),
            dma((2, DOWN_CHUNKS)),
            dma((2, DOWN_CHUNKS)),
            dma((2, DOWN_CHUNKS)),
            dma((2, DOWN_CHUNKS)),
            dma((2,)),
            dma((DOWN_CHUNKS,)),
            dma((DOWN_CHUNKS,)),
            dma((2, ATT_PARTS)),
            dma((2, ATT_PARTS)),
            dma((2, ATT_PARTS)),
            dma((2, ATT_PARTS)),
            dma((2, ATT_PARTS)),
            dma((2, ATT_PARTS)),
        ],
        compiler_params=pltpu.CompilerParams(
            collective_id=0, has_side_effects=True, vmem_limit_bytes=44 * 1024 * 1024
        ),
    )(
        *(
            pltpu.with_memory_space_constraint(a, pltpu.HBM)
            for a in (
                queries,
                keys_values,
                sink_logits,
                out_weight,
                expert_tokens,
                norm_gain.reshape(1, width),
                routes.T,
                route_weights.T,
                gate_weight,
                up_weight,
                down_weight,
            )
        )
    )


def solution(mesh):
    in_specs = (
        P("ep", "tp"),
        P("ep", "tp"),
        P(),
        P(),
        P(("ep", "tp"), None),
        P(),
        P(("ep", "tp"), None),
        P(("ep", "tp"), None),
        P("ep", None, "tp"),
        P("ep", None, "tp"),
        P("ep", "tp", None),
    )
    out_specs = (P(("ep", "tp"), None), P(("ep", "tp"), None))
    return jax.shard_map(body, mesh=mesh, in_specs=in_specs, out_specs=out_specs, check_vma=False)
```

```python
import functools

import jax
import jax.numpy as jnp
from jax import lax
from jax.experimental import pallas as pl
from jax.experimental.pallas import tpu as pltpu
from jax.sharding import PartitionSpec as P

MESH = pl.DeviceIdType.MESH
HEAD_DIM = 64
WINDOW = 128
CAP = 24
SIDE = 4
STEP = 13
F32 = jnp.float32
BF16 = jnp.bfloat16
NEG_FILL = -1e30

GU_CHUNKS = 4
COLUMNS = (128, 128, 256, 256, 256, 256, 256, 256, 128, 128)
DOWN_CHUNKS = len(COLUMNS)
ATT_PARTS = 2


def kernel(
    n_ep,
    n_tp,
    q_hbm,
    kv_hbm,
    sink_hbm,
    ow_hbm,
    tok_hbm,
    gain_hbm,
    routes_hbm,
    rw_hbm,
    g_hbm,
    u_hbm,
    d_hbm,
    mix_ref,
    exp_ref,
    sink_ref,
    gain_ref,
    routes_ref,
    rw_ref,
    q_v,
    kv_v,
    ow_v,
    tok_v,
    normed_v,
    slots_v,
    comb_v,
    out_v,
    arr_v,
    gu_v,
    down_v,
    hid_v,
    back_v,
    ret_v,
    att_v,
    attin_v,
    pass_v,
    acc_v,
    news_sem,
    loc_sem,
    halo_ssem,
    halo_rsem,
    gu_ssem,
    gu_rsem,
    gur_ssem,
    gur_rsem,
    dn_ssem,
    dn_rsem,
    dnr_ssem,
    dnr_rsem,
    disp_sem,
    ret_ssem,
    ret_rsem,
    far_ssem,
    far_rsem,
    fwd_ssem,
    fwd_rsem,
    att_ssem,
    att_rsem,
):
    ep = lax.axis_index("ep")
    tp = lax.axis_index("tp")
    right = lax.rem(tp + 1, n_tp)
    left = lax.rem(tp + n_tp - 1, n_tp)
    next_ep = lax.rem(ep + 1, n_ep)
    prev_ep = lax.rem(ep + n_ep - 1, n_ep)
    rows = q_v.shape[0]
    width = tok_v.shape[1]
    half = width // 2
    hid = gu_v.shape[3]
    starts = [sum(COLUMNS[:c]) for c in range(DOWN_CHUNKS)]
    slot_rows = n_ep * CAP

    def of_width(c):
        return pl.ds(starts[c], COLUMNS[c])

    def local(src, dst, k):
        return pltpu.make_async_copy(src, dst, loc_sem.at[k])

    loads = [
        local(tok_hbm, tok_v, 0),
        local(q_hbm, q_v, 1),
        local(kv_hbm, kv_v.at[pl.ds(WINDOW, rows)], 2),
        local(g_hbm.at[0], gu_v.at[0, 0], 3),
        local(u_hbm.at[0], gu_v.at[0, 1], 4),
        local(ow_hbm, ow_v, 5),
        local(gain_hbm, gain_ref, 6),
        local(routes_hbm, routes_ref, 7),
        local(rw_hbm, rw_ref, 8),
        local(sink_hbm, sink_ref, 9),
    ]
    for c in range(DOWN_CHUNKS):
        loads.append(local(d_hbm.at[0, :, of_width(c)], down_v.at[c, pl.ds(0, hid), pl.ds(0, COLUMNS[c])], 10 + c))
    barrier = pltpu.get_barrier_semaphore()

    def greet(semaphore, device):
        pl.semaphore_signal(semaphore, inc=1, device_id=device, device_id_type=MESH)

    def turn(device):
        y = lax.rem(device // 2, SIDE)
        return (device // (2 * SIDE) + jnp.minimum(y, SIDE - 2)) * n_ep + device

    mine = turn(ep)
    greet(barrier, (ep, right))
    greet(barrier, (ep, left))

    def greet_later(d, count):
        to = lax.rem(ep + d, n_ep)
        later = turn(to) > mine

        @pl.when(later)
        def _():
            greet(barrier, (to, tp))

        return count + jnp.where(later, 1, 0)

    later_count = lax.fori_loop(1, n_ep, greet_later, 0)
    for copy in loads:
        copy.start()
    pl.semaphore_wait(barrier, 2 + n_ep - 1 - later_count)

    def remote(src, dst, ssem, rsem, device):
        return pltpu.make_async_remote_copy(
            src_ref=src,
            dst_ref=dst,
            send_sem=ssem,
            recv_sem=rsem,
            device_id=device,
            device_id_type=MESH,
        )

    halos = [
        remote(
            kv_hbm.at[pl.ds(rows - WINDOW, WINDOW)],
            kv_v.at[pl.ds(0, WINDOW)],
            halo_ssem.at[0],
            halo_rsem.at[0],
            (next_ep, tp),
        ),
        remote(
            kv_hbm.at[pl.ds(0, WINDOW)],
            kv_v.at[pl.ds(WINDOW + rows, WINDOW)],
            halo_ssem.at[1],
            halo_rsem.at[1],
            (prev_ep, tp),
        ),
    ]
    def gu_own(side, k):
        which = k % 2
        part = (k // 2 + side) % 2
        src = (g_hbm, u_hbm)[which].at[0, pl.ds(part * half, half)]
        dst = gu_v.at[1 + side, which, pl.ds(part * half, half)]
        return remote(
            src, dst, gu_ssem.at[side, k], gu_rsem.at[side, k], (ep, (right, left)[side])
        )

    def gu_relay(side, k):
        src = gu_v.at[1 + side, k, pl.ds(side * half, half)]
        dst = gu_v.at[3, k, pl.ds(side * half, half)]
        return remote(
            src, dst, gur_ssem.at[side, k], gur_rsem.at[side, k], (ep, (right, left)[side])
        )

    def dn_own(side, c):
        src = d_hbm.at[0, :, of_width(c)]
        dst = down_v.at[c, pl.ds((1 + side) * hid, hid), pl.ds(0, COLUMNS[c])]
        return remote(
            src, dst, dn_ssem.at[side, c], dn_rsem.at[side, c], (ep, (right, left)[side])
        )

    def dn_relay(side, c):
        at = side * (hid // 2)
        src = down_v.at[c, pl.ds((1 + side) * hid + at, hid // 2), pl.ds(0, COLUMNS[c])]
        dst = down_v.at[c, pl.ds(3 * hid + at, hid // 2), pl.ds(0, COLUMNS[c])]
        return remote(
            src, dst, dnr_ssem.at[side, c], dnr_rsem.at[side, c], (ep, (right, left)[side])
        )

    opposite = lax.rem(tp + 2, n_tp)
    part_rows = att_v.shape[1] // ATT_PARTS
    part_cols = att_v.shape[2] // 2

    def att_far(side, p):
        at = pl.ds(p * part_rows, part_rows)
        src = att_v.at[opposite, at, pl.ds(side * part_cols, part_cols)]
        dst = pass_v.at[side, p]
        return remote(
            src, dst, far_ssem.at[side, p], far_rsem.at[side, p], (ep, (right, left)[side])
        )

    def att_fwd(side, p):
        at = pl.ds(p * part_rows, part_rows)
        dst = attin_v.at[(left, right)[side], at, pl.ds(side * part_cols, part_cols)]
        return remote(
            pass_v.at[side, p],
            dst,
            fwd_ssem.at[side, p],
            fwd_rsem.at[side, p],
            (ep, (right, left)[side]),
        )

    def att_near(side, p):
        at = pl.ds(p * part_rows, part_rows)
        to = (right, left)[side]
        return remote(
            att_v.at[to, at], attin_v.at[tp, at], att_ssem.at[side, p], att_rsem.at[side, p], (ep, to)
        )

    for k in range(GU_CHUNKS):
        for side in range(2):
            gu_own(side, k).start()

    @pl.loop(1, n_ep)
    def _(d):
        to = lax.rem(ep + d, n_ep)

        @pl.when(turn(to) < mine)
        def _():
            greet(news_sem, (to, tp))

    loads[0].wait()
    for k in range(6, 10):
        loads[k].wait()

    @pl.loop(0, 8)
    def _(i):
        at = pl.ds(pl.multiple_of(i * 32, 32), 32)
        x = tok_v[at, :].astype(F32)
        x = x - jnp.mean(x, -1, keepdims=True)
        var = jnp.mean(x * x, -1, keepdims=True)
        normed_v[at, :] = (x * lax.rsqrt(var + 1e-06) * gain_ref[...]).astype(BF16)

    tokens = tok_v.shape[0]
    first = routes_ref[0:1, :]
    second = routes_ref[1:2, :]
    expert_ids = lax.broadcasted_iota(jnp.int32, (n_ep, tokens), 0)
    is_first = expert_ids == first
    is_second = expert_ids == second
    named = is_first | is_second
    before = (
        lax.broadcasted_iota(jnp.int32, (tokens, tokens), 0)
        < lax.broadcasted_iota(jnp.int32, (tokens, tokens), 1)
    ).astype(F32)
    named_f = named.astype(F32)
    rank = jnp.dot(named_f.astype(BF16), before.astype(BF16), preferred_element_type=F32)
    rank = jnp.where(named, rank, -1.0).astype(BF16)
    weight = jnp.where(is_first, rw_ref[0:1, :], 0.0) + jnp.where(is_second, rw_ref[1:2, :], 0.0)
    weight_hi = weight.astype(BF16)
    weight_lo = (weight - weight_hi.astype(F32)).astype(BF16)

    def slot_expert(shape, axis):
        slot = lax.broadcasted_iota(jnp.int32, shape, axis).astype(F32)
        expert = jnp.floor((slot + 0.5) * (1.0 / CAP))
        return expert, slot - expert * CAP

    expert, place = slot_expert((slot_rows, n_ep), 0)
    spread = (expert == lax.broadcasted_iota(jnp.int32, (slot_rows, n_ep), 1).astype(F32)).astype(
        F32
    )
    _, place_t = slot_expert((slot_rows, tokens), 0)
    ranks = jnp.dot(spread.astype(BF16), rank, preferred_element_type=F32)
    slots_v[...] = jnp.where(ranks == place_t, 1.0, 0.0).astype(BF16)

    per_block = 8 * CAP

    @pl.loop(0, slot_rows // per_block)
    def _(i):
        at = pl.ds(pl.multiple_of(i * per_block, per_block), per_block)
        picked = jnp.dot(slots_v[at, :], normed_v[...], preferred_element_type=F32)
        out_v[pl.ds(i * 8, 8)] = picked.astype(BF16).reshape(8, CAP, width)

    @pl.when(later_count > 0)
    def _():
        pl.semaphore_wait(news_sem, later_count)

    for copy in halos:
        copy.start()

    @pl.loop(1, n_ep)
    def _(d):
        to = lax.rem(ep + d * STEP, n_ep)
        remote(out_v.at[to], arr_v.at[ep], disp_sem.at[0], disp_sem.at[1], (to, tp)).start()

    arr_v[ep] = out_v[ep]

    expert_c = jnp.floor((lax.broadcasted_iota(jnp.int32, (n_ep, slot_rows), 1).astype(F32) + 0.5) * (1.0 / CAP))
    spread_t = (
        expert_c == lax.broadcasted_iota(jnp.int32, (n_ep, slot_rows), 0).astype(F32)
    ).astype(F32).astype(BF16)

    def over_slots(table):
        return lax.dot_general(
            table.astype(F32).T.astype(BF16),
            spread_t,
            (((1,), (0,)), ((), ())),
            preferred_element_type=F32,
        )

    _, place_c = slot_expert((tokens, slot_rows), 1)
    chosen = over_slots(rank) == place_c
    comb_v[0] = jnp.where(chosen, over_slots(weight_hi), 0.0).astype(BF16)
    comb_v[1] = jnp.where(chosen, over_slots(weight_lo), 0.0).astype(BF16)

    loads[1].wait()
    loads[2].wait()
    block = 128
    span = block + 2 * WINDOW
    heads = q_v.shape[1] // HEAD_DIM
    blocks_per_dest = rows // block // n_tp
    rel = lax.broadcasted_iota(jnp.int32, (block, span), 1) - lax.broadcasted_iota(
        jnp.int32, (block, span), 0
    )
    key_at = lax.broadcasted_iota(jnp.int32, (block, span), 1)
    seq_total = rows * n_ep

    def attend(b):
        row = pl.multiple_of(b * block, block)
        q = q_v[pl.ds(row, block), :] * jnp.asarray(HEAD_DIM**-0.5, BF16)
        kv = kv_v[pl.ds(row, span), :]
        keys = kv[:, 0:HEAD_DIM]
        values = kv[:, HEAD_DIM : 2 * HEAD_DIM]
        key_pos = key_at + (ep * rows + row - WINDOW)
        allowed = (rel >= 0) & (rel <= 2 * WINDOW) & (key_pos >= 0) & (key_pos < seq_total)
        outs = []
        for h in range(heads):
            sink = sink_ref[tp * heads + h]
            scores = lax.dot_general(
                q[:, h * HEAD_DIM : (h + 1) * HEAD_DIM],
                keys,
                (((1,), (1,)), ((), ())),
                preferred_element_type=F32,
            )
            scores = jnp.where(allowed, scores, NEG_FILL)
            top = jnp.maximum(jnp.max(scores, -1, keepdims=True), sink)
            expo = jnp.exp(scores - top)
            denom = jnp.sum(expo, -1, keepdims=True) + jnp.exp(sink - top)
            mixed = jnp.dot(expo.astype(BF16), values, preferred_element_type=F32)
            outs.append((mixed / denom).astype(BF16))
        att_v[b // blocks_per_dest, pl.ds(pl.multiple_of(lax.rem(b, blocks_per_dest) * block, block), block), :] = (
            jnp.concatenate(outs, axis=1)
        )

    blocks = rows // block

    @pl.loop(1, blocks - 1)
    def _(b):
        attend(b)

    for copy in halos:
        copy.wait_recv()

    @pl.loop(0, 2)
    def _(i):
        attend(i * (blocks - 1))

    for k in range(2):
        for side in range(2):
            gu_own(side, k).wait_recv()
            gu_relay(side, k).start()
    for c in range(2):
        for side in range(2):
            dn_own(side, c).start()

    arrived = arr_v.at[pl.ds(0, n_ep - 1)]
    pltpu.make_async_copy(arrived, arrived, disp_sem.at[1]).wait()

    def widen(s):
        @pl.loop(0, slot_rows // per_block)
        def _(i):
            x = arr_v[pl.ds(i * 8, 8)].reshape(per_block, width)
            g = jnp.dot(x, gu_v[s, 0], preferred_element_type=F32)
            u = jnp.dot(x, gu_v[s, 1], preferred_element_type=F32)
            at = pl.ds(pl.multiple_of(i * per_block, per_block), per_block)
            hid_v[s, at, :] = (g / (1.0 + jnp.exp(-g)) * u).astype(BF16)

    loads[3].wait()
    loads[4].wait()
    widen(0)
    for k in range(2, GU_CHUNKS):
        for side in range(2):
            gu_own(side, k).wait_recv()

    @pl.loop(1, 3)
    def _(s):
        widen(s)

    for k in range(2):
        for side in range(2):
            gu_relay(side, k).wait_recv()
    widen(3)

    def combine(c):
        cols = COLUMNS[c]
        got = ret_v.at[c, pl.ds(0, n_ep - 1), :, pl.ds(0, cols)]
        pltpu.make_async_copy(got, got, ret_rsem.at[c]).wait()
        results = ret_v[c, :, :, 0:cols].reshape(slot_rows, cols)
        total = jnp.dot(comb_v[0], results, preferred_element_type=F32) + jnp.dot(
            comb_v[1], results, preferred_element_type=F32
        )
        exp_ref[:, of_width(c)] = total.astype(BF16)

    def down_sent(c):
        for side in range(2):
            dn_own(side, c).wait_send()
            dn_relay(side, c).wait_send()

    def returned(c):
        sent = back_v.at[c, pl.ds(0, n_ep - 1), :, pl.ds(0, COLUMNS[c])]
        pltpu.make_async_copy(sent, sent, ret_ssem.at[c]).wait()

    def both_ways(send, p):
        for side in range(2):
            send(side, p).start()

    def pass_on(c):
        for side in range(2):
            dn_own(side, c).wait_recv()
            dn_relay(side, c).start()
        if c + 2 < DOWN_CHUNKS:
            for side in range(2):
                dn_own(side, c + 2).start()
        if c + 2 == DOWN_CHUNKS:
            both_ways(att_far, 0)
        if c + 1 == DOWN_CHUNKS:
            both_ways(att_far, 1)
            for p in range(ATT_PARTS):
                both_ways(att_near, p)

    pass_on(0)
    for c in range(DOWN_CHUNKS):
        loads[10 + c].wait()
        for side in range(2):
            dn_relay(side, c).wait_recv()
        if c + 1 < DOWN_CHUNKS:
            pass_on(c + 1)

        cols = COLUMNS[c]
        span_cols = pl.ds(0, cols)

        @pl.loop(0, slot_rows // per_block)
        def _(i):
            at = pl.ds(pl.multiple_of(i * per_block, per_block), per_block)
            total = jnp.zeros((per_block, cols), F32)
            for s in range(4):
                total = total + jnp.dot(
                    hid_v[s, at, :],
                    down_v[c, s * hid : (s + 1) * hid, 0:cols],
                    preferred_element_type=F32,
                )
            back_v[c, pl.ds(i * 8, 8), :, 0:cols] = total.astype(BF16).reshape(8, CAP, cols)

        @pl.loop(1, n_ep)
        def _(d):
            to = lax.rem(ep + d * STEP, n_ep)
            remote(
                back_v.at[c, to, :, span_cols],
                ret_v.at[c, ep, :, span_cols],
                ret_ssem.at[c],
                ret_rsem.at[c],
                (to, tp),
            ).start()

        ret_v[c, ep, :, 0:cols] = back_v[c, ep, :, 0:cols]
        if 5 <= c < DOWN_CHUNKS - 1:
            combine(c - 5)
        if c == 1:
            for copy in halos:
                copy.wait_send()
            for side in range(2):
                for k in range(GU_CHUNKS):
                    gu_own(side, k).wait_send()
                for k in range(2):
                    gu_relay(side, k).wait_send()
        if c == 2:
            sent = out_v.at[pl.ds(0, n_ep - 1)]
            pltpu.make_async_copy(sent, sent, disp_sem.at[0]).wait()
        if c >= 3:
            down_sent(c - 3)

    for p in range(ATT_PARTS):
        for side in range(2):
            att_far(side, p).wait_recv()
            att_fwd(side, p).start()
    for c in range(DOWN_CHUNKS - 3, DOWN_CHUNKS):
        down_sent(c)
    combine(DOWN_CHUNKS - 6)
    for c in range(DOWN_CHUNKS - 5):
        returned(c)

    loads[5].wait()
    head_cols = heads * HEAD_DIM
    mcol = mix_ref.shape[1] // 4

    def add_heads(p, sources, first):
        at = pl.ds(p * part_rows, part_rows)
        for n in range(4):
            cols = pl.ds(n * mcol, mcol)
            total = jnp.zeros((part_rows, mcol), F32) if first else acc_v[at, cols]
            for heads_of, source in sources:
                total = total + jnp.dot(
                    source[at, :],
                    ow_v[pl.ds(pl.multiple_of(heads_of * head_cols, head_cols), head_cols), cols],
                    preferred_element_type=F32,
                )
            if first:
                acc_v[at, cols] = total
            else:
                mix_ref[at, cols] = total.astype(BF16)

    def project_near(p):
        for side in range(2):
            att_near(side, p).wait_recv()
        add_heads(p, ((left, attin_v.at[left]), (right, attin_v.at[right]), (tp, att_v.at[tp])), True)

    def project_far(p):
        for side in range(2):
            att_fwd(side, p).wait_recv()
        add_heads(p, ((opposite, attin_v.at[opposite]),), False)

    combine(DOWN_CHUNKS - 5)
    project_near(0)
    combine(DOWN_CHUNKS - 4)
    project_near(1)
    combine(DOWN_CHUNKS - 3)
    for p in range(ATT_PARTS):
        project_far(p)
    combine(DOWN_CHUNKS - 2)

    for side in range(2):
        for p in range(ATT_PARTS):
            att_far(side, p).wait_send()
            att_fwd(side, p).wait_send()
            att_near(side, p).wait_send()
    for c in range(DOWN_CHUNKS - 5, DOWN_CHUNKS):
        returned(c)
    combine(DOWN_CHUNKS - 1)


def body(
    queries,
    keys_values,
    sink_logits,
    out_weight,
    expert_tokens,
    norm_gain,
    routes,
    route_weights,
    gate_weight,
    up_weight,
    down_weight,
):
    n_ep = lax.axis_size("ep")
    n_tp = lax.axis_size("tp")
    rows, q_cols = queries.shape
    tokens, width = expert_tokens.shape
    hid = gate_weight.shape[2]
    out_rows = rows // n_tp
    dcol = max(COLUMNS)
    slot_rows = n_ep * CAP
    hbm = pl.BlockSpec(memory_space=pltpu.HBM)
    vmem = pl.BlockSpec(memory_space=pltpu.VMEM)
    dma = pltpu.SemaphoreType.DMA
    return pl.pallas_call(
        functools.partial(kernel, n_ep, n_tp),
        out_shape=(
            pltpu.VMEM((out_rows, width), BF16),
            pltpu.VMEM((tokens, width), BF16),
        ),
        in_specs=[hbm] * 11,
        out_specs=(vmem, vmem),
        scratch_shapes=[
            pltpu.SMEM(sink_logits.shape, F32),
            pltpu.VMEM((1, width), F32),
            pltpu.VMEM((2, tokens), jnp.int32),
            pltpu.VMEM((2, tokens), F32),
            pltpu.VMEM((rows, q_cols), BF16),
            pltpu.VMEM((rows + 2 * WINDOW, 2 * HEAD_DIM), BF16),
            pltpu.VMEM(out_weight.shape, BF16),
            pltpu.VMEM((tokens, width), BF16),
            pltpu.VMEM((tokens, width), BF16),
            pltpu.VMEM((slot_rows, tokens), BF16),
            pltpu.VMEM((2, tokens, slot_rows), BF16),
            pltpu.VMEM((n_ep, CAP, width), BF16),
            pltpu.VMEM((n_ep, CAP, width), BF16),
            pltpu.VMEM((4, 2, width, hid), BF16),
            pltpu.VMEM((DOWN_CHUNKS, 4 * hid, dcol), BF16),
            pltpu.VMEM((4, slot_rows, hid), BF16),
            pltpu.VMEM((DOWN_CHUNKS, n_ep, CAP, dcol), BF16),
            pltpu.VMEM((DOWN_CHUNKS, n_ep, CAP, dcol), BF16),
            pltpu.VMEM((n_tp, out_rows, q_cols), BF16),
            pltpu.VMEM((n_tp, out_rows, q_cols), BF16),
            pltpu.VMEM((2, ATT_PARTS, out_rows // ATT_PARTS, q_cols // 2), BF16),
            pltpu.VMEM((out_rows, width), F32),
            pltpu.SemaphoreType.REGULAR,
            dma((10 + DOWN_CHUNKS,)),
            dma((2,)),
            dma((2,)),
            dma((2, GU_CHUNKS)),
            dma((2, GU_CHUNKS)),
            dma((2, 2)),
            dma((2, 2)),
            dma((2, DOWN_CHUNKS)),
            dma((2, DOWN_CHUNKS)),
            dma((2, DOWN_CHUNKS)),
            dma((2, DOWN_CHUNKS)),
            dma((2,)),
            dma((DOWN_CHUNKS,)),
            dma((DOWN_CHUNKS,)),
            dma((2, ATT_PARTS)),
            dma((2, ATT_PARTS)),
            dma((2, ATT_PARTS)),
            dma((2, ATT_PARTS)),
            dma((2, ATT_PARTS)),
            dma((2, ATT_PARTS)),
        ],
        compiler_params=pltpu.CompilerParams(
            collective_id=0, has_side_effects=True, vmem_limit_bytes=52 * 1024 * 1024
        ),
    )(
        *(
            pltpu.with_memory_space_constraint(a, pltpu.HBM)
            for a in (
                queries,
                keys_values,
                sink_logits,
                out_weight,
                expert_tokens,
                norm_gain.reshape(1, width),
                routes.T,
                route_weights.T,
                gate_weight,
                up_weight,
                down_weight,
            )
        )
    )


def solution(mesh):
    in_specs = (
        P("ep", "tp"),
        P("ep", "tp"),
        P(),
        P(),
        P(("ep", "tp"), None),
        P(),
        P(("ep", "tp"), None),
        P(("ep", "tp"), None),
        P("ep", None, "tp"),
        P("ep", None, "tp"),
        P("ep", "tp", None),
    )
    out_specs = (P(("ep", "tp"), None), P(("ep", "tp"), None))
    return jax.shard_map(body, mesh=mesh, in_specs=in_specs, out_specs=out_specs, check_vma=False)
```

```python
import functools

import jax
import jax.numpy as jnp
from jax import lax
from jax.experimental import pallas as pl
from jax.experimental.pallas import tpu as pltpu
from jax.sharding import PartitionSpec as P

MESH = pl.DeviceIdType.MESH
HEAD_DIM = 64
WINDOW = 128
CAP = 24
SIDE = 4
STEP = 13
F32 = jnp.float32
BF16 = jnp.bfloat16
NEG_FILL = -1e30

GU_CHUNKS = 4
COLUMNS = (256,) * 8
DOWN_CHUNKS = len(COLUMNS)
ATT_PARTS = 2


def kernel(
    n_ep,
    n_tp,
    q_hbm,
    kv_hbm,
    sink_hbm,
    ow_hbm,
    tok_hbm,
    gain_hbm,
    routes_hbm,
    rw_hbm,
    g_hbm,
    u_hbm,
    d_hbm,
    mix_ref,
    exp_ref,
    sink_ref,
    gain_ref,
    routes_ref,
    rw_ref,
    q_v,
    kv_v,
    ow_v,
    tok_v,
    normed_v,
    slots_v,
    comb_v,
    out_v,
    arr_v,
    gu_v,
    down_v,
    hid_v,
    back_v,
    ret_v,
    att_v,
    attin_v,
    pass_v,
    acc_v,
    silu_v,
    news_sem,
    loc_sem,
    halo_sem,
    sent_sem,
    gu_sem,
    gur_sem,
    dn_sem,
    dnr_sem,
    disp_sem,
    ret_sem,
    far_sem,
    fwd_sem,
    near_sem,
):
    ep = lax.axis_index("ep")
    tp = lax.axis_index("tp")
    right = lax.rem(tp + 1, n_tp)
    left = lax.rem(tp + n_tp - 1, n_tp)
    next_ep = lax.rem(ep + 1, n_ep)
    prev_ep = lax.rem(ep + n_ep - 1, n_ep)
    rows = q_v.shape[0]
    width = tok_v.shape[1]
    half = width // 2
    hid = gu_v.shape[3]
    starts = [sum(COLUMNS[:c]) for c in range(DOWN_CHUNKS)]
    slot_rows = n_ep * CAP

    def of_width(c):
        return pl.ds(starts[c], COLUMNS[c])

    def local(src, dst, k):
        return pltpu.make_async_copy(src, dst, loc_sem.at[k])

    loads = [
        local(tok_hbm, tok_v, 0),
        local(q_hbm, q_v, 1),
        local(kv_hbm, kv_v.at[pl.ds(WINDOW, rows)], 2),
        local(g_hbm.at[0], gu_v.at[0, 0], 3),
        local(u_hbm.at[0], gu_v.at[0, 1], 4),
        local(ow_hbm, ow_v, 5),
        local(gain_hbm, gain_ref, 6),
        local(routes_hbm, routes_ref, 7),
        local(rw_hbm, rw_ref, 8),
        local(sink_hbm, sink_ref, 9),
    ]
    for c in range(DOWN_CHUNKS):
        loads.append(local(d_hbm.at[0, :, of_width(c)], down_v.at[c, pl.ds(0, hid), pl.ds(0, COLUMNS[c])], 10))
    barrier = pltpu.get_barrier_semaphore()

    def greet(semaphore, device):
        pl.semaphore_signal(semaphore, inc=1, device_id=device, device_id_type=MESH)

    def turn(device):
        y = lax.rem(device // 2, SIDE)
        return (device // (2 * SIDE) + jnp.minimum(y, SIDE - 2)) * n_ep + device

    mine = turn(ep)
    greet(barrier, (ep, right))
    greet(barrier, (ep, left))

    def greet_later(d, count):
        to = lax.rem(ep + d, n_ep)
        later = turn(to) > mine

        @pl.when(later)
        def _():
            greet(barrier, (to, tp))

        return count + jnp.where(later, 1, 0)

    later_count = lax.fori_loop(1, n_ep, greet_later, 0)
    for copy in loads:
        copy.start()
    pl.semaphore_wait(barrier, 2 + n_ep - 1 - later_count)

    def remote(src, dst, ssem, rsem, device):
        return pltpu.make_async_remote_copy(
            src_ref=src,
            dst_ref=dst,
            send_sem=ssem,
            recv_sem=rsem,
            device_id=device,
            device_id_type=MESH,
        )

    def take(like, semaphore):
        pltpu.make_async_copy(like, like, semaphore).wait()

    def both_ways(send, p):
        for side in range(2):
            send(side, p).start()

    halos = [
        remote(
            kv_hbm.at[pl.ds(rows - WINDOW, WINDOW)],
            kv_v.at[pl.ds(0, WINDOW)],
            halo_sem.at[0],
            halo_sem.at[1],
            (next_ep, tp),
        ),
        remote(
            kv_hbm.at[pl.ds(0, WINDOW)],
            kv_v.at[pl.ds(WINDOW + rows, WINDOW)],
            halo_sem.at[0],
            halo_sem.at[1],
            (prev_ep, tp),
        ),
    ]
    def gu_own(side, k):
        which = k % 2
        part = (k // 2 + side) % 2
        src = (g_hbm, u_hbm)[which].at[0, pl.ds(part * half, half)]
        dst = gu_v.at[1 + side, which, pl.ds(part * half, half)]
        return remote(
            src, dst, sent_sem.at[0], gu_sem.at[k], (ep, (right, left)[side])
        )

    def gu_relay(side, k):
        src = gu_v.at[1 + side, k, pl.ds(side * half, half)]
        dst = gu_v.at[3, k, pl.ds(side * half, half)]
        return remote(
            src, dst, sent_sem.at[1], gur_sem.at[k], (ep, (right, left)[side])
        )

    def dn_own(side, c):
        src = d_hbm.at[0, :, of_width(c)]
        dst = down_v.at[c, pl.ds((1 + side) * hid, hid), pl.ds(0, COLUMNS[c])]
        return remote(
            src, dst, sent_sem.at[2], dn_sem.at[c], (ep, (right, left)[side])
        )

    def dn_relay(side, c):
        at = side * (hid // 2)
        src = down_v.at[c, pl.ds((1 + side) * hid + at, hid // 2), pl.ds(0, COLUMNS[c])]
        dst = down_v.at[c, pl.ds(3 * hid + at, hid // 2), pl.ds(0, COLUMNS[c])]
        return remote(
            src, dst, sent_sem.at[3], dnr_sem.at[c], (ep, (right, left)[side])
        )

    opposite = lax.rem(tp + 2, n_tp)
    part_rows = att_v.shape[1] // ATT_PARTS
    part_cols = att_v.shape[2] // 2

    def att_far(side, p):
        at = pl.ds(p * part_rows, part_rows)
        src = att_v.at[opposite, at, pl.ds(side * part_cols, part_cols)]
        dst = pass_v.at[side, p]
        return remote(
            src, dst, sent_sem.at[4], far_sem.at[p], (ep, (right, left)[side])
        )

    def att_fwd(side, p):
        at = pl.ds(p * part_rows, part_rows)
        dst = attin_v.at[(left, right)[side], at, pl.ds(side * part_cols, part_cols)]
        return remote(
            pass_v.at[side, p],
            dst,
            sent_sem.at[5],
            fwd_sem.at[p],
            (ep, (right, left)[side]),
        )

    def att_near(side, p):
        at = pl.ds(p * part_rows, part_rows)
        to = (right, left)[side]
        return remote(
            att_v.at[to, at], attin_v.at[tp, at], sent_sem.at[6], near_sem.at[p], (ep, to)
        )

    for k in range(GU_CHUNKS):
        both_ways(gu_own, k)
    both_ways(dn_own, 0)

    @pl.loop(1, n_ep)
    def _(d):
        to = lax.rem(ep + d, n_ep)

        @pl.when(turn(to) < mine)
        def _():
            greet(news_sem, (to, tp))

    loads[0].wait()
    for k in range(6, 10):
        loads[k].wait()

    @pl.loop(0, 8)
    def _(i):
        at = pl.ds(pl.multiple_of(i * 32, 32), 32)
        x = tok_v[at, :].astype(F32)
        x = x - jnp.mean(x, -1, keepdims=True)
        var = jnp.mean(x * x, -1, keepdims=True)
        normed_v[at, :] = (x * lax.rsqrt(var + 1e-06) * gain_ref[...]).astype(BF16)

    tokens = tok_v.shape[0]
    first = routes_ref[0:1, :]
    second = routes_ref[1:2, :]
    expert_ids = lax.broadcasted_iota(jnp.int32, (n_ep, tokens), 0)
    is_first = expert_ids == first
    is_second = expert_ids == second
    named = is_first | is_second
    before = (
        lax.broadcasted_iota(jnp.int32, (tokens, tokens), 0)
        < lax.broadcasted_iota(jnp.int32, (tokens, tokens), 1)
    ).astype(F32)
    named_f = named.astype(F32)
    rank = jnp.dot(named_f.astype(BF16), before.astype(BF16), preferred_element_type=F32)
    rank = jnp.where(named, rank, -1.0).astype(BF16)
    weight = jnp.where(is_first, rw_ref[0:1, :], 0.0) + jnp.where(is_second, rw_ref[1:2, :], 0.0)
    weight_hi = weight.astype(BF16)
    weight_lo = (weight - weight_hi.astype(F32)).astype(BF16)

    def slot_expert(shape, axis):
        slot = lax.broadcasted_iota(jnp.int32, shape, axis).astype(F32)
        expert = jnp.floor((slot + 0.5) * (1.0 / CAP))
        return expert, slot - expert * CAP

    expert, place = slot_expert((slot_rows, n_ep), 0)
    spread = (expert == lax.broadcasted_iota(jnp.int32, (slot_rows, n_ep), 1).astype(F32)).astype(
        F32
    )
    _, place_t = slot_expert((slot_rows, tokens), 0)
    ranks = jnp.dot(spread.astype(BF16), rank, preferred_element_type=F32)
    slots_v[...] = jnp.where(ranks == place_t, 1.0, 0.0).astype(BF16)

    per_block = 8 * CAP

    @pl.loop(0, slot_rows // per_block)
    def _(i):
        at = pl.ds(pl.multiple_of(i * per_block, per_block), per_block)
        picked = jnp.dot(slots_v[at, :], normed_v[...], preferred_element_type=F32)
        out_v[pl.ds(i * 8, 8)] = picked.astype(BF16).reshape(8, CAP, width)

    @pl.when(later_count > 0)
    def _():
        pl.semaphore_wait(news_sem, later_count)

    for copy in halos:
        copy.start()

    @pl.loop(1, n_ep)
    def _(d):
        to = lax.rem(ep + d * STEP, n_ep)
        remote(out_v.at[to], arr_v.at[ep], disp_sem.at[0], disp_sem.at[1], (to, tp)).start()

    arr_v[ep] = out_v[ep]

    expert_c = jnp.floor((lax.broadcasted_iota(jnp.int32, (n_ep, slot_rows), 1).astype(F32) + 0.5) * (1.0 / CAP))
    spread_t = (
        expert_c == lax.broadcasted_iota(jnp.int32, (n_ep, slot_rows), 0).astype(F32)
    ).astype(F32).astype(BF16)

    def over_slots(table):
        return lax.dot_general(
            table.astype(F32).T.astype(BF16),
            spread_t,
            (((1,), (0,)), ((), ())),
            preferred_element_type=F32,
        )

    _, place_c = slot_expert((tokens, slot_rows), 1)
    chosen = over_slots(rank) == place_c
    comb_v[0] = jnp.where(chosen, over_slots(weight_hi), 0.0).astype(BF16)
    comb_v[1] = jnp.where(chosen, over_slots(weight_lo), 0.0).astype(BF16)

    loads[1].wait()
    loads[2].wait()
    block = 128
    span = block + 2 * WINDOW
    heads = q_v.shape[1] // HEAD_DIM
    blocks_per_dest = rows // block // n_tp
    rel = lax.broadcasted_iota(jnp.int32, (block, span), 1) - lax.broadcasted_iota(
        jnp.int32, (block, span), 0
    )
    key_at = lax.broadcasted_iota(jnp.int32, (block, span), 1)
    seq_total = rows * n_ep

    def attend(b):
        row = pl.multiple_of(b * block, block)
        q = q_v[pl.ds(row, block), :] * jnp.asarray(HEAD_DIM**-0.5, BF16)
        kv = kv_v[pl.ds(row, span), :]
        keys = kv[:, 0:HEAD_DIM]
        values = kv[:, HEAD_DIM : 2 * HEAD_DIM]
        key_pos = key_at + (ep * rows + row - WINDOW)
        allowed = (rel >= 0) & (rel <= 2 * WINDOW) & (key_pos >= 0) & (key_pos < seq_total)
        outs = []
        for h in range(heads):
            sink = sink_ref[tp * heads + h]
            scores = lax.dot_general(
                q[:, h * HEAD_DIM : (h + 1) * HEAD_DIM],
                keys,
                (((1,), (1,)), ((), ())),
                preferred_element_type=F32,
            )
            scores = jnp.where(allowed, scores, NEG_FILL)
            top = jnp.maximum(jnp.max(scores, -1, keepdims=True), sink)
            expo = jnp.exp(scores - top)
            denom = jnp.sum(expo, -1, keepdims=True) + jnp.exp(sink - top)
            mixed = jnp.dot(expo.astype(BF16), values, preferred_element_type=F32)
            outs.append((mixed / denom).astype(BF16))
        att_v[b // blocks_per_dest, pl.ds(pl.multiple_of(lax.rem(b, blocks_per_dest) * block, block), block), :] = (
            jnp.concatenate(outs, axis=1)
        )

    blocks = rows // block

    @pl.loop(1, blocks - 1)
    def _(b):
        attend(b)

    halo_like = kv_v.at[pl.ds(0, 2 * WINDOW)]
    take(halo_like, halo_sem.at[1])

    @pl.loop(0, 2)
    def _(i):
        attend(i * (blocks - 1))

    for k in range(2):
        take(gu_v.at[1, 0], gu_sem.at[k])
        both_ways(gu_relay, k)

    arrived = arr_v.at[pl.ds(0, n_ep - 1)]
    pltpu.make_async_copy(arrived, arrived, disp_sem.at[1]).wait()

    slot_blocks = slot_rows // per_block

    def pass_on(c):
        take(down_v.at[c, pl.ds(hid, 2 * hid), pl.ds(0, COLUMNS[c])], dn_sem.at[c])
        both_ways(dn_relay, c)
        if c == 0:
            both_ways(dn_own, 1)
        if c + 2 < DOWN_CHUNKS:
            both_ways(dn_own, c + 2)

    def widen(s):
        @pl.loop(0, slot_blocks)
        def _(i):
            x = arr_v[pl.ds(i * 8, 8)].reshape(per_block, width)
            g = jnp.dot(x, gu_v[s, 0], preferred_element_type=F32)
            u = jnp.dot(x, gu_v[s, 1], preferred_element_type=F32)
            at = pl.ds(pl.multiple_of(i * per_block, per_block), per_block)
            hid_v[s, at, :] = (g / (1.0 + jnp.exp(-g)) * u).astype(BF16)

    loads[3].wait()
    loads[4].wait()
    widen(0)
    for k in range(2, GU_CHUNKS):
        take(gu_v.at[1, 0], gu_sem.at[k])

    pass_on(0)

    @pl.loop(1, 3)
    def _(s):
        widen(s)

    take(gu_v.at[3, 0], gur_sem.at[0])

    @pl.loop(0, slot_blocks)
    def _(i):
        x = arr_v[pl.ds(i * 8, 8)].reshape(per_block, width)
        g = jnp.dot(x, gu_v[3, 0], preferred_element_type=F32)
        at = pl.ds(pl.multiple_of(i * per_block, per_block), per_block)
        silu_v[at, :] = g / (1.0 + jnp.exp(-g))

    take(halo_like, halo_sem.at[0])
    take(gu_v.at[pl.ds(0, 2)], sent_sem.at[0])
    sent = out_v.at[pl.ds(0, n_ep - 1)]
    take(sent, disp_sem.at[0])
    take(gu_v.at[0, 0], loc_sem.at[10])
    take(gu_v.at[3, 1], gur_sem.at[1])

    @pl.loop(0, slot_blocks)
    def _(i):
        x = arr_v[pl.ds(i * 8, 8)].reshape(per_block, width)
        u = jnp.dot(x, gu_v[3, 1], preferred_element_type=F32)
        at = pl.ds(pl.multiple_of(i * per_block, per_block), per_block)
        hid_v[3, at, :] = (silu_v[at, :] * u).astype(BF16)

    take(gu_v.at[0], sent_sem.at[1])

    def combine(c):
        cols = COLUMNS[c]
        got = ret_v.at[c, pl.ds(0, n_ep - 1), :, pl.ds(0, cols)]
        take(got, ret_sem.at[c])
        results = ret_v[c, :, :, 0:cols].reshape(slot_rows, cols)
        total = jnp.dot(comb_v[0], results, preferred_element_type=F32) + jnp.dot(
            comb_v[1], results, preferred_element_type=F32
        )
        exp_ref[:, of_width(c)] = total.astype(BF16)

    for c in range(DOWN_CHUNKS):
        if 0 < c < DOWN_CHUNKS - 1:
            pass_on(c + 1)
        take(down_v.at[c, pl.ds(3 * hid, hid), pl.ds(0, COLUMNS[c])], dnr_sem.at[c])

        cols = COLUMNS[c]
        span_cols = pl.ds(0, cols)

        @pl.loop(0, slot_rows // per_block)
        def _(i):
            at = pl.ds(pl.multiple_of(i * per_block, per_block), per_block)
            total = jnp.zeros((per_block, cols), F32)
            for s in range(4):
                total = total + jnp.dot(
                    hid_v[s, at, :],
                    down_v[c, s * hid : (s + 1) * hid, 0:cols],
                    preferred_element_type=F32,
                )
            back_v[c, pl.ds(i * 8, 8), :, 0:cols] = total.astype(BF16).reshape(8, CAP, cols)

        @pl.loop(1, n_ep)
        def _(d):
            to = lax.rem(ep + d * STEP, n_ep)
            remote(
                back_v.at[c, to, :, span_cols],
                ret_v.at[c, ep, :, span_cols],
                sent_sem.at[7],
                ret_sem.at[c],
                (to, tp),
            ).start()

        ret_v[c, ep, :, 0:cols] = back_v[c, ep, :, 0:cols]
        if c == 0:
            pass_on(1)
        if c == DOWN_CHUNKS - 2:
            for send in (att_far, att_near):
                for p in range(ATT_PARTS):
                    both_ways(send, p)
        if 4 <= c < DOWN_CHUNKS - 1:
            combine(c - 4)

    for p in range(ATT_PARTS):
        take(pass_v.at[:, p], far_sem.at[p])
        both_ways(att_fwd, p)
    take(gu_v.at[0], sent_sem.at[2])
    take(gu_v.at[0, 0], sent_sem.at[3])

    loads[5].wait()
    head_cols = heads * HEAD_DIM
    mcol = mix_ref.shape[1] // 4

    def add_heads(p, sources, first):
        at = pl.ds(p * part_rows, part_rows)
        for n in range(4):
            cols = pl.ds(n * mcol, mcol)
            total = jnp.zeros((part_rows, mcol), F32) if first else acc_v[at, cols]
            for heads_of, source in sources:
                total = total + jnp.dot(
                    source[at, :],
                    ow_v[pl.ds(pl.multiple_of(heads_of * head_cols, head_cols), head_cols), cols],
                    preferred_element_type=F32,
                )
            if first:
                acc_v[at, cols] = total
            else:
                mix_ref[at, cols] = total.astype(BF16)

    def project_near(p):
        take(attin_v.at[pl.ds(0, 2), pl.ds(p * part_rows, part_rows)], near_sem.at[p])
        add_heads(p, ((left, attin_v.at[left]), (right, attin_v.at[right]), (tp, att_v.at[tp])), True)

    def project_far(p):
        take(attin_v.at[opposite, pl.ds(p * part_rows, part_rows)], fwd_sem.at[p])
        add_heads(p, ((opposite, attin_v.at[opposite]),), False)

    combine(DOWN_CHUNKS - 5)
    project_near(0)
    combine(DOWN_CHUNKS - 4)
    project_near(1)
    combine(DOWN_CHUNKS - 3)
    for p in range(ATT_PARTS):
        project_far(p)
    combine(DOWN_CHUNKS - 2)

    take(attin_v.at[0], sent_sem.at[4])
    take(attin_v.at[0], sent_sem.at[5])
    take(attin_v.at[pl.ds(0, 2)], sent_sem.at[6])
    combine(DOWN_CHUNKS - 1)
    take(sent, sent_sem.at[7])


def put_out(mix_ref, exp_ref, mix_hbm, exp_hbm, sem):
    copies = [
        pltpu.make_async_copy(mix_ref, mix_hbm, sem.at[0]),
        pltpu.make_async_copy(exp_ref, exp_hbm, sem.at[1]),
    ]
    for copy in copies:
        copy.start()
    for copy in copies:
        copy.wait()


def body(
    queries,
    keys_values,
    sink_logits,
    out_weight,
    expert_tokens,
    norm_gain,
    routes,
    route_weights,
    gate_weight,
    up_weight,
    down_weight,
):
    n_ep = lax.axis_size("ep")
    n_tp = lax.axis_size("tp")
    rows, q_cols = queries.shape
    tokens, width = expert_tokens.shape
    hid = gate_weight.shape[2]
    out_rows = rows // n_tp
    dcol = max(COLUMNS)
    slot_rows = n_ep * CAP
    hbm = pl.BlockSpec(memory_space=pltpu.HBM)
    vmem = pl.BlockSpec(memory_space=pltpu.VMEM)
    dma = pltpu.SemaphoreType.DMA
    held = pl.pallas_call(
        functools.partial(kernel, n_ep, n_tp),
        out_shape=(
            pltpu.VMEM((out_rows, width), BF16),
            pltpu.VMEM((tokens, width), BF16),
        ),
        in_specs=[hbm] * 11,
        out_specs=(vmem, vmem),
        scratch_shapes=[
            pltpu.SMEM(sink_logits.shape, F32),
            pltpu.VMEM((1, width), F32),
            pltpu.VMEM((2, tokens), jnp.int32),
            pltpu.VMEM((2, tokens), F32),
            pltpu.VMEM((rows, q_cols), BF16),
            pltpu.VMEM((rows + 2 * WINDOW, 2 * HEAD_DIM), BF16),
            pltpu.VMEM(out_weight.shape, BF16),
            pltpu.VMEM((tokens, width), BF16),
            pltpu.VMEM((tokens, width), BF16),
            pltpu.VMEM((slot_rows, tokens), BF16),
            pltpu.VMEM((2, tokens, slot_rows), BF16),
            pltpu.VMEM((n_ep, CAP, width), BF16),
            pltpu.VMEM((n_ep, CAP, width), BF16),
            pltpu.VMEM((4, 2, width, hid), BF16),
            pltpu.VMEM((DOWN_CHUNKS, 4 * hid, dcol), BF16),
            pltpu.VMEM((4, slot_rows, hid), BF16),
            pltpu.VMEM((DOWN_CHUNKS, n_ep, CAP, dcol), BF16),
            pltpu.VMEM((DOWN_CHUNKS, n_ep, CAP, dcol), BF16),
            pltpu.VMEM((n_tp, out_rows, q_cols), BF16),
            pltpu.VMEM((n_tp, out_rows, q_cols), BF16),
            pltpu.VMEM((2, ATT_PARTS, out_rows // ATT_PARTS, q_cols // 2), BF16),
            pltpu.VMEM((out_rows, width), F32),
            pltpu.VMEM((slot_rows, hid), F32),
            pltpu.SemaphoreType.REGULAR,
            dma((11,)),
            dma((2,)),
            dma((8,)),
            dma((GU_CHUNKS,)),
            dma((2,)),
            dma((DOWN_CHUNKS,)),
            dma((DOWN_CHUNKS,)),
            dma((2,)),
            dma((DOWN_CHUNKS,)),
            dma((ATT_PARTS,)),
            dma((ATT_PARTS,)),
            dma((ATT_PARTS,)),
        ],
        compiler_params=pltpu.CompilerParams(
            collective_id=0, has_side_effects=True, vmem_limit_bytes=52 * 1024 * 1024
        ),
    )(
        *(
            pltpu.with_memory_space_constraint(a, pltpu.HBM)
            for a in (
                queries,
                keys_values,
                sink_logits,
                out_weight,
                expert_tokens,
                norm_gain.reshape(1, width),
                routes.T,
                route_weights.T,
                gate_weight,
                up_weight,
                down_weight,
            )
        )
    )
    return pl.pallas_call(
        put_out,
        out_shape=(
            jax.ShapeDtypeStruct((out_rows, width), BF16),
            jax.ShapeDtypeStruct((tokens, width), BF16),
        ),
        in_specs=[vmem, vmem],
        out_specs=(pl.BlockSpec(memory_space=pl.ANY),) * 2,
        scratch_shapes=[dma((2,))],
        compiler_params=pltpu.CompilerParams(vmem_limit_bytes=1024 * 1024),
    )(*held)


def solution(mesh):
    in_specs = (
        P("ep", "tp"),
        P("ep", "tp"),
        P(),
        P(),
        P(("ep", "tp"), None),
        P(),
        P(("ep", "tp"), None),
        P(("ep", "tp"), None),
        P("ep", None, "tp"),
        P("ep", None, "tp"),
        P("ep", "tp", None),
    )
    out_specs = (P(("ep", "tp"), None), P(("ep", "tp"), None))
    return jax.shard_map(body, mesh=mesh, in_specs=in_specs, out_specs=out_specs, check_vma=False)
```

```python
import functools

import jax
import jax.numpy as jnp
from jax import lax
from jax.experimental import pallas as pl
from jax.experimental.pallas import tpu as pltpu
from jax.sharding import PartitionSpec as P

MESH = pl.DeviceIdType.MESH
HEAD_DIM = 64
WINDOW = 128
CAP = 24
SIDE = 4
STEP = 13
F32 = jnp.float32
BF16 = jnp.bfloat16
NEG_FILL = -1e30

GU_CHUNKS = 4
COLUMNS = (256,) * 8
DOWN_CHUNKS = len(COLUMNS)
ATT_PARTS = 2


def kernel(
    n_ep,
    n_tp,
    q_hbm,
    kv_hbm,
    sink_hbm,
    ow_hbm,
    tok_hbm,
    gain_hbm,
    routes_hbm,
    rw_hbm,
    g_hbm,
    u_hbm,
    d_hbm,
    mix_ref,
    exp_ref,
    sink_ref,
    gain_ref,
    routes_ref,
    rw_ref,
    q_v,
    kv_v,
    ow_v,
    tok_v,
    normed_v,
    slots_v,
    comb_v,
    out_v,
    arr_v,
    gu_v,
    down_v,
    hid_v,
    back_v,
    ret_v,
    att_v,
    attin_v,
    pass_v,
    acc_v,
    silu_v,
    part_v,
    sum_v,
    got_v,
    news_sem,
    loc_sem,
    halo_sem,
    sent_sem,
    gu_sem,
    gur_sem,
    dn_sem,
    dnr_sem,
    disp_sem,
    ret_sem,
    far_sem,
    fwd_sem,
    near_sem,
    tok_sem,
    part_sem,
):
    ep = lax.axis_index("ep")
    tp = lax.axis_index("tp")
    right = lax.rem(tp + 1, n_tp)
    left = lax.rem(tp + n_tp - 1, n_tp)
    next_ep = lax.rem(ep + 1, n_ep)
    prev_ep = lax.rem(ep + n_ep - 1, n_ep)
    rows = q_v.shape[0]
    width = tok_v.shape[2]
    parity = lax.rem(tp, 2)
    at_site = lax.rem(ep, 2) == parity
    off_site = lax.rem(ep, 2) != parity
    partner = jnp.where(at_site, right, left)
    served = n_ep // 2
    place = ep // 2
    half = width // 2
    hid = gu_v.shape[3]
    starts = [sum(COLUMNS[:c]) for c in range(DOWN_CHUNKS)]
    slot_rows = 2 * n_ep * CAP
    table_rows = served * CAP

    def of_width(c):
        return pl.ds(starts[c], COLUMNS[c])

    def local(src, dst, k):
        return pltpu.make_async_copy(src, dst, loc_sem.at[k])

    loads = [
        local(tok_hbm, tok_v.at[0], 0),
        local(q_hbm, q_v, 1),
        local(kv_hbm, kv_v.at[pl.ds(WINDOW, rows)], 2),
        local(g_hbm.at[0], gu_v.at[0, 0], 3),
        local(u_hbm.at[0], gu_v.at[0, 1], 4),
        local(ow_hbm, ow_v, 5),
        local(gain_hbm, gain_ref, 6),
        local(routes_hbm, routes_ref.at[0], 7),
        local(rw_hbm, rw_ref.at[0], 8),
        local(sink_hbm, sink_ref, 9),
    ]
    for c in range(DOWN_CHUNKS):
        loads.append(local(d_hbm.at[0, :, of_width(c)], down_v.at[c, pl.ds(0, hid), pl.ds(0, COLUMNS[c])], 10))
    barrier = pltpu.get_barrier_semaphore()

    def greet(semaphore, device):
        pl.semaphore_signal(semaphore, inc=1, device_id=device, device_id_type=MESH)

    def turn(device):
        y = lax.rem(device // 2, SIDE)
        return (device // (2 * SIDE) + jnp.minimum(y, SIDE - 2)) * n_ep + device

    mine = turn(ep)
    greet(barrier, (ep, right))
    greet(barrier, (ep, left))

    def greet_later(d, count):
        to = lax.rem(ep + d, n_ep)
        later = turn(to) > mine

        @pl.when(later)
        def _():
            greet(barrier, (to, tp))

        return count + jnp.where(later, 1, 0)

    later_count = lax.fori_loop(1, n_ep, greet_later, 0)
    for copy in loads:
        copy.start()
    pl.semaphore_wait(barrier, 2 + n_ep - 1 - later_count)

    def remote(src, dst, ssem, rsem, device):
        return pltpu.make_async_remote_copy(
            src_ref=src,
            dst_ref=dst,
            send_sem=ssem,
            recv_sem=rsem,
            device_id=device,
            device_id_type=MESH,
        )

    def take(like, semaphore):
        pltpu.make_async_copy(like, like, semaphore).wait()

    def both_ways(send, p):
        for side in range(2):
            send(side, p).start()

    halos = [
        remote(
            kv_hbm.at[pl.ds(rows - WINDOW, WINDOW)],
            kv_v.at[pl.ds(0, WINDOW)],
            halo_sem.at[0],
            halo_sem.at[1],
            (next_ep, tp),
        ),
        remote(
            kv_hbm.at[pl.ds(0, WINDOW)],
            kv_v.at[pl.ds(WINDOW + rows, WINDOW)],
            halo_sem.at[0],
            halo_sem.at[1],
            (prev_ep, tp),
        ),
    ]
    def gu_own(side, k):
        which = k % 2
        part = (k // 2 + side) % 2
        src = (g_hbm, u_hbm)[which].at[0, pl.ds(part * half, half)]
        dst = gu_v.at[1 + side, which, pl.ds(part * half, half)]
        return remote(
            src, dst, sent_sem.at[0], gu_sem.at[k], (ep, (right, left)[side])
        )

    def gu_relay(side, k):
        src = gu_v.at[1 + side, k, pl.ds(side * half, half)]
        dst = gu_v.at[3, k, pl.ds(side * half, half)]
        return remote(
            src, dst, sent_sem.at[1], gur_sem.at[k], (ep, (right, left)[side])
        )

    def dn_own(side, c):
        src = d_hbm.at[0, :, of_width(c)]
        dst = down_v.at[c, pl.ds((1 + side) * hid, hid), pl.ds(0, COLUMNS[c])]
        return remote(
            src, dst, sent_sem.at[2], dn_sem.at[c], (ep, (right, left)[side])
        )

    def dn_half(side, c):
        at = side * (hid // 2)
        src = d_hbm.at[0, pl.ds(at, hid // 2), of_width(c)]
        dst = down_v.at[c, pl.ds((1 + side) * hid + at, hid // 2), pl.ds(0, COLUMNS[c])]
        return remote(src, dst, sent_sem.at[2], dn_sem.at[c], (ep, (right, left)[side]))

    def dn_relay(side, c):
        at = side * (hid // 2)
        src = down_v.at[c, pl.ds((1 + side) * hid + at, hid // 2), pl.ds(0, COLUMNS[c])]
        dst = down_v.at[c, pl.ds(3 * hid + at, hid // 2), pl.ds(0, COLUMNS[c])]
        return remote(
            src, dst, sent_sem.at[3], dnr_sem.at[c], (ep, (right, left)[side])
        )

    opposite = lax.rem(tp + 2, n_tp)
    part_rows = att_v.shape[1] // ATT_PARTS
    part_cols = att_v.shape[2] // 2

    def att_far(side, p):
        at = pl.ds(p * part_rows, part_rows)
        src = att_v.at[opposite, at, pl.ds(side * part_cols, part_cols)]
        dst = pass_v.at[side, p]
        return remote(
            src, dst, sent_sem.at[4], far_sem.at[p], (ep, (right, left)[side])
        )

    def att_fwd(side, p):
        at = pl.ds(p * part_rows, part_rows)
        dst = attin_v.at[(left, right)[side], at, pl.ds(side * part_cols, part_cols)]
        return remote(
            pass_v.at[side, p],
            dst,
            sent_sem.at[5],
            fwd_sem.at[p],
            (ep, (right, left)[side]),
        )

    def att_near(side, p):
        at = pl.ds(p * part_rows, part_rows)
        to = (right, left)[side]
        return remote(
            att_v.at[to, at], attin_v.at[tp, at], sent_sem.at[6], near_sem.at[p], (ep, to)
        )

    exchange = [
        remote(routes_hbm, routes_ref.at[1], sent_sem.at[8], tok_sem.at[0], (ep, partner)),
        remote(rw_hbm, rw_ref.at[1], sent_sem.at[9], tok_sem.at[1], (ep, partner)),
        remote(tok_hbm, tok_v.at[1], sent_sem.at[10], tok_sem.at[2], (ep, partner)),
    ]
    for copy in exchange:
        copy.start()
    @pl.loop(1, n_ep)
    def _(d):
        to = lax.rem(ep + d, n_ep)

        @pl.when(turn(to) < mine)
        def _():
            greet(news_sem, (to, tp))

    tokens = tok_v.shape[1]
    per_block = 8 * CAP

    def slot_expert(shape, axis):
        slot = lax.broadcasted_iota(jnp.int32, shape, axis).astype(F32)
        expert = jnp.floor((slot + 0.5) * (1.0 / CAP))
        return expert, slot - expert * CAP

    def tables(b):
        @pl.loop(0, 8)
        def _(i):
            at = pl.ds(pl.multiple_of(i * 32, 32), 32)
            x = tok_v[b, at, :].astype(F32)
            x = x - jnp.mean(x, -1, keepdims=True)
            var = jnp.mean(x * x, -1, keepdims=True)
            normed_v[b, at, :] = (x * lax.rsqrt(var + 1e-06) * gain_ref[...]).astype(BF16)

        expert_ids = lax.broadcasted_iota(jnp.int32, (served, tokens), 0) * 2 + parity
        is_first = expert_ids == routes_ref[b, 0:1, :]
        is_second = expert_ids == routes_ref[b, 1:2, :]
        named = is_first | is_second
        before = (
            lax.broadcasted_iota(jnp.int32, (tokens, tokens), 0)
            < lax.broadcasted_iota(jnp.int32, (tokens, tokens), 1)
        ).astype(F32)
        rank = jnp.dot(
            named.astype(F32).astype(BF16), before.astype(BF16), preferred_element_type=F32
        )
        rank = jnp.where(named, rank, -1.0)
        weight = jnp.where(is_first, rw_ref[b, 0:1, :], 0.0) + jnp.where(
            is_second, rw_ref[b, 1:2, :], 0.0
        )

        expert, _ = slot_expert((table_rows, served), 0)
        spread = (
            expert == lax.broadcasted_iota(jnp.int32, (table_rows, served), 1).astype(F32)
        ).astype(F32)
        _, place_t = slot_expert((table_rows, tokens), 0)
        ranks = jnp.dot(spread.astype(BF16), rank.astype(BF16), preferred_element_type=F32)
        slots_v[b] = jnp.where(ranks == place_t, 1.0, 0.0).astype(BF16)

        @pl.loop(0, table_rows // per_block)
        def _(i):
            at = pl.ds(pl.multiple_of(i * per_block, per_block), per_block)
            picked = jnp.dot(slots_v[b, at, :], normed_v[b], preferred_element_type=F32)
            out_v[pl.ds(i * 8, 8), b] = picked.astype(BF16).reshape(8, CAP, width)

        return rank, weight

    def dispatch(b):
        @pl.loop(0, served)
        def _(d):
            expert = lax.rem(place + d * STEP, served)
            to = expert * 2 + parity

            @pl.when(to != ep)
            def _():
                remote(
                    out_v.at[expert, b], arr_v.at[ep, b], sent_sem.at[11 + b], disp_sem.at[b], (to, tp)
                ).start()

        @pl.when(at_site)
        def _():
            arr_v[ep, b] = out_v[place, b]

    def combine_table(b, rank, weight):
        expert_c, _ = slot_expert((served, table_rows), 1)
        spread_t = (
            expert_c == lax.broadcasted_iota(jnp.int32, (served, table_rows), 0).astype(F32)
        ).astype(F32).astype(BF16)

        def over_slots(table):
            return jnp.dot(table.T.astype(BF16), spread_t, preferred_element_type=F32)

        _, place_c = slot_expert((tokens, table_rows), 1)
        chosen = over_slots(rank) == place_c
        weight_hi = weight.astype(BF16).astype(F32)
        comb_v[b, 0] = jnp.where(chosen, over_slots(weight_hi), 0.0).astype(BF16)
        comb_v[b, 1] = jnp.where(chosen, over_slots(weight - weight_hi), 0.0).astype(BF16)

    loads[0].wait()
    for k in range(6, 10):
        loads[k].wait()
    own_tables = tables(0)

    @pl.when(later_count > 0)
    def _():
        pl.semaphore_wait(news_sem, later_count)

    for copy in halos:
        copy.start()
    dispatch(0)

    for k in range(2):
        both_ways(gu_own, k)

    @pl.when(off_site)
    def _():
        for k in range(2, GU_CHUNKS):
            both_ways(gu_own, k)

    @pl.when(at_site)
    def _():
        for c in range(DOWN_CHUNKS):
            both_ways(dn_half, c)

    combine_table(0, *own_tables)

    loads[1].wait()
    loads[2].wait()
    block = 128
    span = block + 2 * WINDOW
    heads = q_v.shape[1] // HEAD_DIM
    blocks_per_dest = rows // block // n_tp
    rel = lax.broadcasted_iota(jnp.int32, (block, span), 1) - lax.broadcasted_iota(
        jnp.int32, (block, span), 0
    )
    key_at = lax.broadcasted_iota(jnp.int32, (block, span), 1)
    seq_total = rows * n_ep

    def attend(b):
        row = pl.multiple_of(b * block, block)
        q = q_v[pl.ds(row, block), :] * jnp.asarray(HEAD_DIM**-0.5, BF16)
        kv = kv_v[pl.ds(row, span), :]
        keys = kv[:, 0:HEAD_DIM]
        values = kv[:, HEAD_DIM : 2 * HEAD_DIM]
        key_pos = key_at + (ep * rows + row - WINDOW)
        allowed = (rel >= 0) & (rel <= 2 * WINDOW) & (key_pos >= 0) & (key_pos < seq_total)
        outs = []
        for h in range(heads):
            sink = sink_ref[tp * heads + h]
            scores = lax.dot_general(
                q[:, h * HEAD_DIM : (h + 1) * HEAD_DIM],
                keys,
                (((1,), (1,)), ((), ())),
                preferred_element_type=F32,
            )
            scores = jnp.where(allowed, scores, NEG_FILL)
            top = jnp.maximum(jnp.max(scores, -1, keepdims=True), sink)
            expo = jnp.exp(scores - top)
            denom = jnp.sum(expo, -1, keepdims=True) + jnp.exp(sink - top)
            mixed = jnp.dot(expo.astype(BF16), values, preferred_element_type=F32)
            outs.append((mixed / denom).astype(BF16))
        att_v[b // blocks_per_dest, pl.ds(pl.multiple_of(lax.rem(b, blocks_per_dest) * block, block), block), :] = (
            jnp.concatenate(outs, axis=1)
        )

    blocks = rows // block

    @pl.loop(1, 5)
    def _(b):
        attend(b)

    for copy in exchange:
        copy.wait_recv()
    partner_tables = tables(1)
    dispatch(1)
    combine_table(1, *partner_tables)

    @pl.loop(5, blocks - 1)
    def _(b):
        attend(b)

    halo_like = kv_v.at[pl.ds(0, 2 * WINDOW)]
    take(halo_like, halo_sem.at[1])

    @pl.loop(0, 2)
    def _(i):
        attend(i * (blocks - 1))

    def send_attended():
        for send in (att_far, att_near):
            for p in range(ATT_PARTS):
                both_ways(send, p)

    @pl.when(off_site)
    def _():
        for k in range(2):
            take(gu_v.at[1, 0], gu_sem.at[k])
            both_ways(gu_relay, k)
        for c in range(DOWN_CHUNKS):
            both_ways(dn_own, c)
            take(down_v.at[c, pl.ds(0, hid), pl.ds(0, COLUMNS[c])], dn_sem.at[c])
            both_ways(dn_relay, c)
        send_attended()

    big_block = 16 * CAP
    slot_blocks = slot_rows // big_block

    def sources(i):
        return pl.ds(lax.rem(i, 2) * 16, 16)

    def arrived(i):
        return arr_v[sources(i), i // 2].reshape(big_block, width)

    def rows_of(i):
        return pl.ds(pl.multiple_of(i * big_block, big_block), big_block)

    def widen(s, first=0, last=slot_blocks):
        @pl.loop(first, last)
        def _(i):
            x = arrived(i)
            g = jnp.dot(x, gu_v[s, 0], preferred_element_type=F32)
            u = jnp.dot(x, gu_v[s, 1], preferred_element_type=F32)
            at = rows_of(i)
            hid_v[s, at, :] = (g / (1.0 + jnp.exp(-g)) * u).astype(BF16)

    loads[3].wait()
    loads[4].wait()
    take(gu_v.at[0, 0], loc_sem.at[10])

    def part_copy(c):
        return remote(
            part_v.at[c], got_v.at[c], sent_sem.at[13], part_sem.at[c], (ep, partner)
        )

    def combine(c):
        cols = COLUMNS[c]

        @pl.when(at_site)
        def _():
            take(ret_v.at[c, pl.ds(0, served - 1)], ret_sem.at[c])

        @pl.when(off_site)
        def _():
            take(ret_v.at[c], ret_sem.at[c])

        def share(b):
            results = ret_v[c, :, b].reshape(table_rows, cols)
            return jnp.dot(comb_v[b, 0], results, preferred_element_type=F32) + jnp.dot(
                comb_v[b, 1], results, preferred_element_type=F32
            )

        part_v[c] = share(1).astype(BF16)
        part_copy(c).start()
        sum_v[c] = share(0)

    def finish(c):
        take(got_v.at[c], part_sem.at[c])
        exp_ref[:, of_width(c)] = (sum_v[c] + got_v[c].astype(F32)).astype(BF16)

    @pl.when(at_site)
    def _():
        for b in range(2):
            take(arr_v.at[pl.ds(0, n_ep - 1), b], disp_sem.at[b])
            widen(0, 2 * b, 2 * b + 2)
        for k in range(GU_CHUNKS):
            take(gu_v.at[1, 0], gu_sem.at[k])

        @pl.loop(1, 3)
        def _(s):
            widen(s)

        take(gu_v.at[3, 0], gur_sem.at[0])

        @pl.loop(0, slot_blocks)
        def _(i):
            g = jnp.dot(arrived(i), gu_v[3, 0], preferred_element_type=F32)
            at = rows_of(i)
            silu_v[at, :] = g / (1.0 + jnp.exp(-g))

        take(gu_v.at[3, 1], gur_sem.at[1])

        @pl.loop(0, slot_blocks)
        def _(i):
            u = jnp.dot(arrived(i), gu_v[3, 1], preferred_element_type=F32)
            at = rows_of(i)
            hid_v[3, at, :] = (silu_v[at, :] * u).astype(BF16)

        for c in range(DOWN_CHUNKS):
            cols = COLUMNS[c]
            take(down_v.at[c, pl.ds(hid, 2 * hid), pl.ds(0, cols)], dn_sem.at[c])
            take(down_v.at[c, pl.ds(3 * hid, hid), pl.ds(0, cols)], dnr_sem.at[c])

            @pl.loop(0, slot_blocks)
            def _(i):
                at = rows_of(i)
                total = jnp.zeros((big_block, cols), F32)
                for s in range(4):
                    total = total + jnp.dot(
                        hid_v[s, at, :],
                        down_v[c, s * hid : (s + 1) * hid, 0:cols],
                        preferred_element_type=F32,
                    )
                back_v[c, sources(i), i // 2] = total.astype(BF16).reshape(16, CAP, cols)

            @pl.loop(1, n_ep)
            def _(d):
                to = lax.rem(ep + d * STEP, n_ep)
                remote(
                    back_v.at[c, to], ret_v.at[c, place], sent_sem.at[7], ret_sem.at[c], (to, tp)
                ).start()

            ret_v[c, place] = back_v[c, ep]
            if c == 4:
                send_attended()
            if c >= 5:
                combine(c - 5)

    @pl.when(off_site)
    def _():
        for c in range(3):
            combine(c)

    for p in range(ATT_PARTS):
        take(pass_v.at[:, p], far_sem.at[p])
        both_ways(att_fwd, p)

    loads[5].wait()
    head_cols = heads * HEAD_DIM
    mcol = mix_ref.shape[1] // 4

    def add_heads(p, sources, first):
        at = pl.ds(p * part_rows, part_rows)
        for n in range(4):
            cols = pl.ds(n * mcol, mcol)
            total = jnp.zeros((part_rows, mcol), F32) if first else acc_v[at, cols]
            for heads_of, source in sources:
                total = total + jnp.dot(
                    source[at, :],
                    ow_v[pl.ds(pl.multiple_of(heads_of * head_cols, head_cols), head_cols), cols],
                    preferred_element_type=F32,
                )
            if first:
                acc_v[at, cols] = total
            else:
                mix_ref[at, cols] = total.astype(BF16)

    def project_near(p):
        take(attin_v.at[pl.ds(0, 2), pl.ds(p * part_rows, part_rows)], near_sem.at[p])
        add_heads(p, ((left, attin_v.at[left]), (right, attin_v.at[right]), (tp, att_v.at[tp])), True)

    def project_far(p):
        take(attin_v.at[opposite, pl.ds(p * part_rows, part_rows)], fwd_sem.at[p])
        add_heads(p, ((opposite, attin_v.at[opposite]),), False)

    combine(3)
    combine(4)
    project_near(0)
    combine(5)
    project_near(1)
    for c in range(4):
        finish(c)
    combine(6)
    for p in range(ATT_PARTS):
        project_far(p)
    for c in range(4, 6):
        finish(c)
    combine(7)

    take(kv_v.at[pl.ds(0, 2 * WINDOW)], halo_sem.at[0])
    for copy in exchange:
        copy.wait_send()

    @pl.when(at_site)
    def _():
        take(gu_v.at[0], sent_sem.at[0])
        take(gu_v.at[0, 0], sent_sem.at[2])
        for b in range(2):
            take(out_v.at[pl.ds(0, served - 1), b], sent_sem.at[11 + b])
        for c in range(DOWN_CHUNKS):
            take(back_v.at[c, pl.ds(0, n_ep - 1)], sent_sem.at[7])

    @pl.when(off_site)
    def _():
        take(gu_v.at[pl.ds(0, 2)], sent_sem.at[0])
        take(gu_v.at[0], sent_sem.at[1])
        take(gu_v.at[0], sent_sem.at[2])
        take(gu_v.at[0, 0], sent_sem.at[3])
        for b in range(2):
            take(out_v.at[:, b], sent_sem.at[11 + b])

    take(attin_v.at[0], sent_sem.at[4])
    take(attin_v.at[0], sent_sem.at[5])
    take(attin_v.at[pl.ds(0, 2)], sent_sem.at[6])
    finish(6)
    finish(7)
    take(part_v, sent_sem.at[13])


def put_out(mix_ref, exp_ref, mix_hbm, exp_hbm, sem):
    copies = [
        pltpu.make_async_copy(mix_ref, mix_hbm, sem.at[0]),
        pltpu.make_async_copy(exp_ref, exp_hbm, sem.at[1]),
    ]
    for copy in copies:
        copy.start()
    for copy in copies:
        copy.wait()


def body(
    queries,
    keys_values,
    sink_logits,
    out_weight,
    expert_tokens,
    norm_gain,
    routes,
    route_weights,
    gate_weight,
    up_weight,
    down_weight,
):
    n_ep = lax.axis_size("ep")
    n_tp = lax.axis_size("tp")
    rows, q_cols = queries.shape
    tokens, width = expert_tokens.shape
    hid = gate_weight.shape[2]
    out_rows = rows // n_tp
    dcol = max(COLUMNS)
    served = n_ep // 2
    slot_rows = 2 * n_ep * CAP
    table_rows = served * CAP
    hbm = pl.BlockSpec(memory_space=pltpu.HBM)
    vmem = pl.BlockSpec(memory_space=pltpu.VMEM)
    dma = pltpu.SemaphoreType.DMA
    held = pl.pallas_call(
        functools.partial(kernel, n_ep, n_tp),
        out_shape=(
            pltpu.VMEM((out_rows, width), BF16),
            pltpu.VMEM((tokens, width), BF16),
        ),
        in_specs=[hbm] * 11,
        out_specs=(vmem, vmem),
        scratch_shapes=[
            pltpu.SMEM(sink_logits.shape, F32),
            pltpu.VMEM((1, width), F32),
            pltpu.VMEM((2, 2, tokens), jnp.int32),
            pltpu.VMEM((2, 2, tokens), F32),
            pltpu.VMEM((rows, q_cols), BF16),
            pltpu.VMEM((rows + 2 * WINDOW, 2 * HEAD_DIM), BF16),
            pltpu.VMEM(out_weight.shape, BF16),
            pltpu.VMEM((2, tokens, width), BF16),
            pltpu.VMEM((2, tokens, width), BF16),
            pltpu.VMEM((2, table_rows, tokens), BF16),
            pltpu.VMEM((2, 2, tokens, table_rows), BF16),
            pltpu.VMEM((served, 2, CAP, width), BF16),
            pltpu.VMEM((n_ep, 2, CAP, width), BF16),
            pltpu.VMEM((4, 2, width, hid), BF16),
            pltpu.VMEM((DOWN_CHUNKS, 4 * hid, dcol), BF16),
            pltpu.VMEM((4, slot_rows, hid), BF16),
            pltpu.VMEM((DOWN_CHUNKS, n_ep, 2, CAP, dcol), BF16),
            pltpu.VMEM((DOWN_CHUNKS, served, 2, CAP, dcol), BF16),
            pltpu.VMEM((n_tp, out_rows, q_cols), BF16),
            pltpu.VMEM((n_tp, out_rows, q_cols), BF16),
            pltpu.VMEM((2, ATT_PARTS, out_rows // ATT_PARTS, q_cols // 2), BF16),
            pltpu.VMEM((out_rows, width), F32),
            pltpu.VMEM((slot_rows, hid), F32),
            pltpu.VMEM((DOWN_CHUNKS, tokens, dcol), BF16),
            pltpu.VMEM((DOWN_CHUNKS, tokens, dcol), F32),
            pltpu.VMEM((DOWN_CHUNKS, tokens, dcol), BF16),
            pltpu.SemaphoreType.REGULAR,
            dma((11,)),
            dma((2,)),
            dma((14,)),
            dma((GU_CHUNKS,)),
            dma((2,)),
            dma((DOWN_CHUNKS,)),
            dma((DOWN_CHUNKS,)),
            dma((2,)),
            dma((DOWN_CHUNKS,)),
            dma((ATT_PARTS,)),
            dma((ATT_PARTS,)),
            dma((ATT_PARTS,)),
            dma((3,)),
            dma((DOWN_CHUNKS,)),
        ],
        compiler_params=pltpu.CompilerParams(
            collective_id=0, has_side_effects=True, vmem_limit_bytes=59 * 1024 * 1024
        ),
    )(
        *(
            pltpu.with_memory_space_constraint(a, pltpu.HBM)
            for a in (
                queries,
                keys_values,
                sink_logits,
                out_weight,
                expert_tokens,
                norm_gain.reshape(1, width),
                routes.T,
                route_weights.T,
                gate_weight,
                up_weight,
                down_weight,
            )
        )
    )
    return pl.pallas_call(
        put_out,
        out_shape=(
            jax.ShapeDtypeStruct((out_rows, width), BF16),
            jax.ShapeDtypeStruct((tokens, width), BF16),
        ),
        in_specs=[vmem, vmem],
        out_specs=(pl.BlockSpec(memory_space=pl.ANY),) * 2,
        scratch_shapes=[dma((2,))],
        compiler_params=pltpu.CompilerParams(vmem_limit_bytes=1024 * 1024),
    )(*held)


def solution(mesh):
    in_specs = (
        P("ep", "tp"),
        P("ep", "tp"),
        P(),
        P(),
        P(("ep", "tp"), None),
        P(),
        P(("ep", "tp"), None),
        P(("ep", "tp"), None),
        P("ep", None, "tp"),
        P("ep", None, "tp"),
        P("ep", "tp", None),
    )
    out_specs = (P(("ep", "tp"), None), P(("ep", "tp"), None))
    return jax.shard_map(body, mesh=mesh, in_specs=in_specs, out_specs=out_specs, check_vma=False)
```

```python
import functools

import jax
import jax.numpy as jnp
from jax import lax
from jax.experimental import pallas as pl
from jax.experimental.pallas import tpu as pltpu
from jax.sharding import PartitionSpec as P

MESH = pl.DeviceIdType.MESH
HEAD_DIM = 64
WINDOW = 128
CAP = 24
SIDE = 4
STEP = 7
F32 = jnp.float32
BF16 = jnp.bfloat16
NEG_FILL = -1e30

GU_CHUNKS = 4
COLUMNS = (256,) * 8
DOWN_CHUNKS = len(COLUMNS)
ATT_PARTS = 2
EARLY = 2


def kernel(
    n_ep,
    n_tp,
    q_hbm,
    kv_hbm,
    sink_hbm,
    ow_hbm,
    tok_hbm,
    gain_hbm,
    routes_hbm,
    rw_hbm,
    g_hbm,
    u_hbm,
    d_hbm,
    mix_ref,
    exp_ref,
    sink_ref,
    gain_ref,
    routes_ref,
    rw_ref,
    q_v,
    kv_v,
    ow_v,
    tok_v,
    normed_v,
    slots_v,
    comb_v,
    out_v,
    arr_v,
    gu_v,
    down_v,
    hid_v,
    back_v,
    ret_v,
    att_v,
    attin_v,
    pass_v,
    acc_v,
    silu_v,
    part_v,
    sum_v,
    got_v,
    news_sem,
    loc_sem,
    halo_sem,
    sent_sem,
    gu_sem,
    gur_sem,
    dn_sem,
    dnr_sem,
    disp_sem,
    ret_sem,
    far_sem,
    fwd_sem,
    near_sem,
    tok_sem,
    part_sem,
):
    ep = lax.axis_index("ep")
    tp = lax.axis_index("tp")
    right = lax.rem(tp + 1, n_tp)
    left = lax.rem(tp + n_tp - 1, n_tp)
    next_ep = lax.rem(ep + 1, n_ep)
    prev_ep = lax.rem(ep + n_ep - 1, n_ep)
    rows = q_v.shape[0]
    width = tok_v.shape[2]
    parity = lax.rem(tp, 2)
    at_site = lax.rem(ep, 2) == parity
    off_site = lax.rem(ep, 2) != parity
    partner = jnp.where(at_site, right, left)
    served = n_ep // 2
    place = ep // 2
    half = width // 2
    hid = gu_v.shape[3]
    starts = [sum(COLUMNS[:c]) for c in range(DOWN_CHUNKS)]
    slot_rows = 2 * n_ep * CAP
    table_rows = served * CAP

    def of_width(c):
        return pl.ds(starts[c], COLUMNS[c])

    def local(src, dst, k):
        return pltpu.make_async_copy(src, dst, loc_sem.at[k])

    loads = [
        local(tok_hbm, tok_v.at[0], 0),
        local(q_hbm, q_v, 1),
        local(kv_hbm, kv_v.at[pl.ds(WINDOW, rows)], 2),
        local(g_hbm.at[0], gu_v.at[0, 0], 3),
        local(u_hbm.at[0], gu_v.at[0, 1], 4),
        local(ow_hbm, ow_v, 5),
        local(gain_hbm, gain_ref, 6),
        local(routes_hbm, routes_ref.at[0], 7),
        local(rw_hbm, rw_ref.at[0], 8),
        local(sink_hbm, sink_ref, 9),
    ]
    for c in range(DOWN_CHUNKS):
        loads.append(local(d_hbm.at[0, :, of_width(c)], down_v.at[c, pl.ds(0, hid), pl.ds(0, COLUMNS[c])], 10))
    barrier = pltpu.get_barrier_semaphore()

    def greet(semaphore, device):
        pl.semaphore_signal(semaphore, inc=1, device_id=device, device_id_type=MESH)

    def turn(device):
        y = lax.rem(device // 2, SIDE)
        return (device // (2 * SIDE) + jnp.minimum(y, SIDE - 2)) * n_ep + device

    mine = turn(ep)
    greet(barrier, (ep, right))
    greet(barrier, (ep, left))

    def greet_later(d, count):
        to = lax.rem(ep + d, n_ep)
        later = turn(to) > mine

        @pl.when(later)
        def _():
            greet(barrier, (to, tp))

        return count + jnp.where(later, 1, 0)

    later_count = lax.fori_loop(1, n_ep, greet_later, 0)
    for copy in loads:
        copy.start()
    pl.semaphore_wait(barrier, 2 + n_ep - 1 - later_count)

    def remote(src, dst, ssem, rsem, device):
        return pltpu.make_async_remote_copy(
            src_ref=src,
            dst_ref=dst,
            send_sem=ssem,
            recv_sem=rsem,
            device_id=device,
            device_id_type=MESH,
        )

    def take(like, semaphore):
        pltpu.make_async_copy(like, like, semaphore).wait()

    def both_ways(send, p):
        for side in range(2):
            send(side, p).start()

    halos = [
        remote(
            kv_hbm.at[pl.ds(rows - WINDOW, WINDOW)],
            kv_v.at[pl.ds(0, WINDOW)],
            halo_sem.at[0],
            halo_sem.at[1],
            (next_ep, tp),
        ),
        remote(
            kv_hbm.at[pl.ds(0, WINDOW)],
            kv_v.at[pl.ds(WINDOW + rows, WINDOW)],
            halo_sem.at[0],
            halo_sem.at[1],
            (prev_ep, tp),
        ),
    ]
    def gu_own(side, k):
        which = k % 2
        part = (k // 2 + side) % 2
        src = (g_hbm, u_hbm)[which].at[0, pl.ds(part * half, half)]
        dst = gu_v.at[1 + side, which, pl.ds(part * half, half)]
        return remote(
            src, dst, sent_sem.at[0], gu_sem.at[k], (ep, (right, left)[side])
        )

    def gu_relay(side, k):
        src = gu_v.at[1 + side, k, pl.ds(side * half, half)]
        dst = gu_v.at[3, k, pl.ds(side * half, half)]
        return remote(
            src, dst, sent_sem.at[1], gur_sem.at[k], (ep, (right, left)[side])
        )

    def dn_own(side, c):
        src = d_hbm.at[0, :, of_width(c)]
        dst = down_v.at[c, pl.ds((1 + side) * hid, hid), pl.ds(0, COLUMNS[c])]
        return remote(
            src, dst, sent_sem.at[2], dn_sem.at[c], (ep, (right, left)[side])
        )

    def dn_half(side, c):
        at = side * (hid // 2)
        src = d_hbm.at[0, pl.ds(at, hid // 2), of_width(c)]
        dst = down_v.at[c, pl.ds((1 + side) * hid + at, hid // 2), pl.ds(0, COLUMNS[c])]
        return remote(src, dst, sent_sem.at[2], dn_sem.at[c], (ep, (right, left)[side]))

    def dn_relay(side, c):
        at = side * (hid // 2)
        src = down_v.at[c, pl.ds((1 + side) * hid + at, hid // 2), pl.ds(0, COLUMNS[c])]
        dst = down_v.at[c, pl.ds(3 * hid + at, hid // 2), pl.ds(0, COLUMNS[c])]
        return remote(
            src, dst, sent_sem.at[3], dnr_sem.at[c], (ep, (right, left)[side])
        )

    opposite = lax.rem(tp + 2, n_tp)
    part_rows = att_v.shape[1] // ATT_PARTS
    part_cols = att_v.shape[2] // 2

    def att_far(side, p):
        at = pl.ds(p * part_rows, part_rows)
        src = att_v.at[opposite, at, pl.ds(side * part_cols, part_cols)]
        dst = pass_v.at[side, p]
        return remote(
            src, dst, sent_sem.at[4], far_sem.at[p], (ep, (right, left)[side])
        )

    def att_fwd(side, p):
        at = pl.ds(p * part_rows, part_rows)
        dst = attin_v.at[(left, right)[side], at, pl.ds(side * part_cols, part_cols)]
        return remote(
            pass_v.at[side, p],
            dst,
            sent_sem.at[5],
            fwd_sem.at[p],
            (ep, (right, left)[side]),
        )

    def att_near(side, p):
        at = pl.ds(p * part_rows, part_rows)
        to = (right, left)[side]
        return remote(
            att_v.at[to, at], attin_v.at[tp, at], sent_sem.at[6], near_sem.at[p], (ep, to)
        )

    exchange = [
        remote(routes_hbm, routes_ref.at[1], sent_sem.at[8], tok_sem.at[0], (ep, partner)),
        remote(rw_hbm, rw_ref.at[1], sent_sem.at[9], tok_sem.at[1], (ep, partner)),
        remote(tok_hbm, tok_v.at[1], sent_sem.at[10], tok_sem.at[2], (ep, partner)),
    ]
    for copy in exchange:
        copy.start()
    @pl.loop(1, n_ep)
    def _(d):
        to = lax.rem(ep + d, n_ep)

        @pl.when(turn(to) < mine)
        def _():
            greet(news_sem, (to, tp))

    tokens = tok_v.shape[1]
    per_block = 8 * CAP

    def slot_expert(shape, axis):
        slot = lax.broadcasted_iota(jnp.int32, shape, axis).astype(F32)
        expert = jnp.floor((slot + 0.5) * (1.0 / CAP))
        return expert, slot - expert * CAP

    def tables(b):
        @pl.loop(0, 8)
        def _(i):
            at = pl.ds(pl.multiple_of(i * 32, 32), 32)
            x = tok_v[b, at, :].astype(F32)
            x = x - jnp.mean(x, -1, keepdims=True)
            var = jnp.mean(x * x, -1, keepdims=True)
            normed_v[b, at, :] = (x * lax.rsqrt(var + 1e-06) * gain_ref[...]).astype(BF16)

        expert_ids = lax.broadcasted_iota(jnp.int32, (served, tokens), 0) * 2 + parity
        is_first = expert_ids == routes_ref[b, 0:1, :]
        is_second = expert_ids == routes_ref[b, 1:2, :]
        named = is_first | is_second
        before = (
            lax.broadcasted_iota(jnp.int32, (tokens, tokens), 0)
            < lax.broadcasted_iota(jnp.int32, (tokens, tokens), 1)
        ).astype(F32)
        rank = jnp.dot(
            named.astype(F32).astype(BF16), before.astype(BF16), preferred_element_type=F32
        )
        rank = jnp.where(named, rank, -1.0)
        weight = jnp.where(is_first, rw_ref[b, 0:1, :], 0.0) + jnp.where(
            is_second, rw_ref[b, 1:2, :], 0.0
        )

        expert, _ = slot_expert((table_rows, served), 0)
        spread = (
            expert == lax.broadcasted_iota(jnp.int32, (table_rows, served), 1).astype(F32)
        ).astype(F32)
        _, place_t = slot_expert((table_rows, tokens), 0)
        ranks = jnp.dot(spread.astype(BF16), rank.astype(BF16), preferred_element_type=F32)
        slots_v[b] = jnp.where(ranks == place_t, 1.0, 0.0).astype(BF16)

        @pl.loop(0, table_rows // per_block)
        def _(i):
            at = pl.ds(pl.multiple_of(i * per_block, per_block), per_block)
            picked = jnp.dot(slots_v[b, at, :], normed_v[b], preferred_element_type=F32)
            out_v[pl.ds(i * 8, 8), b] = picked.astype(BF16).reshape(8, CAP, width)

        return rank, weight

    def dispatch(b):
        @pl.loop(0, served)
        def _(d):
            expert = lax.rem(place + d * STEP, served)
            to = expert * 2 + parity

            @pl.when(to != ep)
            def _():
                remote(
                    out_v.at[expert, b], arr_v.at[ep, b], sent_sem.at[11 + b], disp_sem.at[b], (to, tp)
                ).start()

        @pl.when(at_site)
        def _():
            arr_v[ep, b] = out_v[place, b]

    def combine_table(b, rank, weight):
        expert_c, _ = slot_expert((served, table_rows), 1)
        spread_t = (
            expert_c == lax.broadcasted_iota(jnp.int32, (served, table_rows), 0).astype(F32)
        ).astype(F32).astype(BF16)

        def over_slots(table):
            return jnp.dot(table.T.astype(BF16), spread_t, preferred_element_type=F32)

        _, place_c = slot_expert((tokens, table_rows), 1)
        chosen = over_slots(rank) == place_c
        weight_hi = weight.astype(BF16).astype(F32)
        comb_v[b, 0] = jnp.where(chosen, over_slots(weight_hi), 0.0).astype(BF16)
        comb_v[b, 1] = jnp.where(chosen, over_slots(weight - weight_hi), 0.0).astype(BF16)

    loads[0].wait()
    for k in range(6, 10):
        loads[k].wait()
    own_tables = tables(0)

    @pl.when(later_count > 0)
    def _():
        pl.semaphore_wait(news_sem, later_count)

    for copy in halos:
        copy.start()
    dispatch(0)

    combine_table(0, *own_tables)

    loads[1].wait()
    loads[2].wait()
    block = 128
    span = block + 2 * WINDOW
    heads = q_v.shape[1] // HEAD_DIM
    blocks_per_dest = rows // block // n_tp
    rel = lax.broadcasted_iota(jnp.int32, (block, span), 1) - lax.broadcasted_iota(
        jnp.int32, (block, span), 0
    )
    key_at = lax.broadcasted_iota(jnp.int32, (block, span), 1)
    seq_total = rows * n_ep

    def attend(b):
        row = pl.multiple_of(b * block, block)
        q = q_v[pl.ds(row, block), :] * jnp.asarray(HEAD_DIM**-0.5, BF16)
        kv = kv_v[pl.ds(row, span), :]
        keys = kv[:, 0:HEAD_DIM]
        values = kv[:, HEAD_DIM : 2 * HEAD_DIM]
        key_pos = key_at + (ep * rows + row - WINDOW)
        allowed = (rel >= 0) & (rel <= 2 * WINDOW) & (key_pos >= 0) & (key_pos < seq_total)
        outs = []
        for h in range(heads):
            sink = sink_ref[tp * heads + h]
            scores = lax.dot_general(
                q[:, h * HEAD_DIM : (h + 1) * HEAD_DIM],
                keys,
                (((1,), (1,)), ((), ())),
                preferred_element_type=F32,
            )
            scores = jnp.where(allowed, scores, NEG_FILL)
            top = jnp.maximum(jnp.max(scores, -1, keepdims=True), sink)
            expo = jnp.exp(scores - top)
            denom = jnp.sum(expo, -1, keepdims=True) + jnp.exp(sink - top)
            mixed = jnp.dot(expo.astype(BF16), values, preferred_element_type=F32)
            outs.append((mixed / denom).astype(BF16))
        att_v[b // blocks_per_dest, pl.ds(pl.multiple_of(lax.rem(b, blocks_per_dest) * block, block), block), :] = (
            jnp.concatenate(outs, axis=1)
        )

    blocks = rows // block

    @pl.loop(1, 3)
    def _(b):
        attend(b)

    for k in range(2):
        both_ways(gu_own, k)

    @pl.when(off_site)
    def _():
        for k in range(2, GU_CHUNKS):
            both_ways(gu_own, k)

    @pl.when(at_site)
    def _():
        for c in range(EARLY):
            both_ways(dn_half, c)

    attend(3)
    for copy in exchange:
        copy.wait_recv()
    partner_tables = tables(1)
    dispatch(1)
    combine_table(1, *partner_tables)

    @pl.loop(4, blocks - 1)
    def _(b):
        attend(b)

    halo_like = kv_v.at[pl.ds(0, 2 * WINDOW)]
    take(halo_like, halo_sem.at[1])

    @pl.loop(0, 2)
    def _(i):
        attend(i * (blocks - 1))

    def send_attended():
        for send in (att_far, att_near):
            for p in range(ATT_PARTS):
                both_ways(send, p)

    @pl.when(off_site)
    def _():
        for k in range(2):
            take(gu_v.at[1, 0], gu_sem.at[k])
            both_ways(gu_relay, k)
        for c in range(DOWN_CHUNKS):
            both_ways(dn_own, c)
            take(down_v.at[c, pl.ds(0, hid), pl.ds(0, COLUMNS[c])], dn_sem.at[c])
            both_ways(dn_relay, c)
        send_attended()

    big_block = 16 * CAP
    slot_blocks = slot_rows // big_block

    def sources(i):
        return pl.ds(lax.rem(i, 2) * 16, 16)

    def arrived(i):
        return arr_v[sources(i), i // 2].reshape(big_block, width)

    def rows_of(i):
        return pl.ds(pl.multiple_of(i * big_block, big_block), big_block)

    def widen(s, first=0, last=slot_blocks):
        @pl.loop(first, last)
        def _(i):
            x = arrived(i)
            g = jnp.dot(x, gu_v[s, 0], preferred_element_type=F32)
            u = jnp.dot(x, gu_v[s, 1], preferred_element_type=F32)
            at = rows_of(i)
            hid_v[s, at, :] = (g / (1.0 + jnp.exp(-g)) * u).astype(BF16)

    loads[3].wait()
    loads[4].wait()
    take(gu_v.at[0, 0], loc_sem.at[10])

    def part_copy(c):
        return remote(
            part_v.at[c], got_v.at[c], sent_sem.at[13], part_sem.at[c], (ep, partner)
        )

    def combine(c):
        cols = COLUMNS[c]

        @pl.when(at_site)
        def _():
            take(ret_v.at[c, pl.ds(0, served - 1)], ret_sem.at[c])

        @pl.when(off_site)
        def _():
            take(ret_v.at[c], ret_sem.at[c])

        def share(b):
            results = ret_v[c, :, b].reshape(table_rows, cols)
            return jnp.dot(comb_v[b, 0], results, preferred_element_type=F32) + jnp.dot(
                comb_v[b, 1], results, preferred_element_type=F32
            )

        part_v[c] = share(1).astype(BF16)
        part_copy(c).start()
        sum_v[c] = share(0)

    def finish(c):
        take(got_v.at[c], part_sem.at[c])
        exp_ref[:, of_width(c)] = (sum_v[c] + got_v[c].astype(F32)).astype(BF16)

    @pl.when(at_site)
    def _():
        for b in range(2):
            take(arr_v.at[pl.ds(0, n_ep - 1), b], disp_sem.at[b])
            widen(0, 2 * b, 2 * b + 2)
        for k in range(GU_CHUNKS):
            take(gu_v.at[1, 0], gu_sem.at[k])

        @pl.loop(1, 3)
        def _(s):
            widen(s)

        for c in range(EARLY, DOWN_CHUNKS):
            both_ways(dn_half, c)

        take(gu_v.at[3, 0], gur_sem.at[0])

        @pl.loop(0, slot_blocks)
        def _(i):
            g = jnp.dot(arrived(i), gu_v[3, 0], preferred_element_type=F32)
            at = rows_of(i)
            silu_v[at, :] = g / (1.0 + jnp.exp(-g))

        take(gu_v.at[3, 1], gur_sem.at[1])

        @pl.loop(0, slot_blocks)
        def _(i):
            u = jnp.dot(arrived(i), gu_v[3, 1], preferred_element_type=F32)
            at = rows_of(i)
            hid_v[3, at, :] = (silu_v[at, :] * u).astype(BF16)

        for c in range(DOWN_CHUNKS):
            cols = COLUMNS[c]
            take(down_v.at[c, pl.ds(hid, 2 * hid), pl.ds(0, cols)], dn_sem.at[c])
            take(down_v.at[c, pl.ds(3 * hid, hid), pl.ds(0, cols)], dnr_sem.at[c])

            @pl.loop(0, slot_blocks)
            def _(i):
                at = rows_of(i)
                total = jnp.zeros((big_block, cols), F32)
                for s in range(4):
                    total = total + jnp.dot(
                        hid_v[s, at, :],
                        down_v[c, s * hid : (s + 1) * hid, 0:cols],
                        preferred_element_type=F32,
                    )
                back_v[c, sources(i), i // 2] = total.astype(BF16).reshape(16, CAP, cols)

            @pl.loop(1, n_ep)
            def _(d):
                to = lax.rem(ep + d * STEP, n_ep)
                remote(
                    back_v.at[c, to], ret_v.at[c, place], sent_sem.at[7], ret_sem.at[c], (to, tp)
                ).start()

            ret_v[c, place] = back_v[c, ep]
            if c == 4:
                send_attended()
            if c >= 5:
                combine(c - 5)

    @pl.when(off_site)
    def _():
        for c in range(3):
            combine(c)

    for p in range(ATT_PARTS):
        take(pass_v.at[:, p], far_sem.at[p])
        both_ways(att_fwd, p)

    loads[5].wait()
    head_cols = heads * HEAD_DIM
    mcol = mix_ref.shape[1] // 4

    def add_heads(p, sources, first):
        at = pl.ds(p * part_rows, part_rows)
        for n in range(4):
            cols = pl.ds(n * mcol, mcol)
            total = jnp.zeros((part_rows, mcol), F32) if first else acc_v[at, cols]
            for heads_of, source in sources:
                total = total + jnp.dot(
                    source[at, :],
                    ow_v[pl.ds(pl.multiple_of(heads_of * head_cols, head_cols), head_cols), cols],
                    preferred_element_type=F32,
                )
            if first:
                acc_v[at, cols] = total
            else:
                mix_ref[at, cols] = total.astype(BF16)

    def project_near(p):
        take(attin_v.at[pl.ds(0, 2), pl.ds(p * part_rows, part_rows)], near_sem.at[p])
        add_heads(p, ((left, attin_v.at[left]), (right, attin_v.at[right]), (tp, att_v.at[tp])), True)

    def project_far(p):
        take(attin_v.at[opposite, pl.ds(p * part_rows, part_rows)], fwd_sem.at[p])
        add_heads(p, ((opposite, attin_v.at[opposite]),), False)

    combine(3)
    combine(4)
    project_near(0)
    combine(5)
    project_near(1)
    for c in range(4):
        finish(c)
    combine(6)
    for p in range(ATT_PARTS):
        project_far(p)
    for c in range(4, 6):
        finish(c)
    combine(7)

    take(kv_v.at[pl.ds(0, 2 * WINDOW)], halo_sem.at[0])
    for copy in exchange:
        copy.wait_send()

    @pl.when(at_site)
    def _():
        take(gu_v.at[0], sent_sem.at[0])
        take(gu_v.at[0, 0], sent_sem.at[2])
        for b in range(2):
            take(out_v.at[pl.ds(0, served - 1), b], sent_sem.at[11 + b])
        for c in range(DOWN_CHUNKS):
            take(back_v.at[c, pl.ds(0, n_ep - 1)], sent_sem.at[7])

    @pl.when(off_site)
    def _():
        take(gu_v.at[pl.ds(0, 2)], sent_sem.at[0])
        take(gu_v.at[0], sent_sem.at[1])
        take(gu_v.at[0], sent_sem.at[2])
        take(gu_v.at[0, 0], sent_sem.at[3])
        for b in range(2):
            take(out_v.at[:, b], sent_sem.at[11 + b])

    take(attin_v.at[0], sent_sem.at[4])
    take(attin_v.at[0], sent_sem.at[5])
    take(attin_v.at[pl.ds(0, 2)], sent_sem.at[6])
    finish(6)
    finish(7)
    take(part_v, sent_sem.at[13])


def put_out(mix_ref, exp_ref, mix_hbm, exp_hbm, sem):
    copies = [
        pltpu.make_async_copy(mix_ref, mix_hbm, sem.at[0]),
        pltpu.make_async_copy(exp_ref, exp_hbm, sem.at[1]),
    ]
    for copy in copies:
        copy.start()
    for copy in copies:
        copy.wait()


def body(
    queries,
    keys_values,
    sink_logits,
    out_weight,
    expert_tokens,
    norm_gain,
    routes,
    route_weights,
    gate_weight,
    up_weight,
    down_weight,
):
    n_ep = lax.axis_size("ep")
    n_tp = lax.axis_size("tp")
    rows, q_cols = queries.shape
    tokens, width = expert_tokens.shape
    hid = gate_weight.shape[2]
    out_rows = rows // n_tp
    dcol = max(COLUMNS)
    served = n_ep // 2
    slot_rows = 2 * n_ep * CAP
    table_rows = served * CAP
    hbm = pl.BlockSpec(memory_space=pltpu.HBM)
    vmem = pl.BlockSpec(memory_space=pltpu.VMEM)
    dma = pltpu.SemaphoreType.DMA
    held = pl.pallas_call(
        functools.partial(kernel, n_ep, n_tp),
        out_shape=(
            pltpu.VMEM((out_rows, width), BF16),
            pltpu.VMEM((tokens, width), BF16),
        ),
        in_specs=[hbm] * 11,
        out_specs=(vmem, vmem),
        scratch_shapes=[
            pltpu.SMEM(sink_logits.shape, F32),
            pltpu.VMEM((1, width), F32),
            pltpu.VMEM((2, 2, tokens), jnp.int32),
            pltpu.VMEM((2, 2, tokens), F32),
            pltpu.VMEM((rows, q_cols), BF16),
            pltpu.VMEM((rows + 2 * WINDOW, 2 * HEAD_DIM), BF16),
            pltpu.VMEM(out_weight.shape, BF16),
            pltpu.VMEM((2, tokens, width), BF16),
            pltpu.VMEM((2, tokens, width), BF16),
            pltpu.VMEM((2, table_rows, tokens), BF16),
            pltpu.VMEM((2, 2, tokens, table_rows), BF16),
            pltpu.VMEM((served, 2, CAP, width), BF16),
            pltpu.VMEM((n_ep, 2, CAP, width), BF16),
            pltpu.VMEM((4, 2, width, hid), BF16),
            pltpu.VMEM((DOWN_CHUNKS, 4 * hid, dcol), BF16),
            pltpu.VMEM((4, slot_rows, hid), BF16),
            pltpu.VMEM((DOWN_CHUNKS, n_ep, 2, CAP, dcol), BF16),
            pltpu.VMEM((DOWN_CHUNKS, served, 2, CAP, dcol), BF16),
            pltpu.VMEM((n_tp, out_rows, q_cols), BF16),
            pltpu.VMEM((n_tp, out_rows, q_cols), BF16),
            pltpu.VMEM((2, ATT_PARTS, out_rows // ATT_PARTS, q_cols // 2), BF16),
            pltpu.VMEM((out_rows, width), F32),
            pltpu.VMEM((slot_rows, hid), F32),
            pltpu.VMEM((DOWN_CHUNKS, tokens, dcol), BF16),
            pltpu.VMEM((DOWN_CHUNKS, tokens, dcol), F32),
            pltpu.VMEM((DOWN_CHUNKS, tokens, dcol), BF16),
            pltpu.SemaphoreType.REGULAR,
            dma((11,)),
            dma((2,)),
            dma((14,)),
            dma((GU_CHUNKS,)),
            dma((2,)),
            dma((DOWN_CHUNKS,)),
            dma((DOWN_CHUNKS,)),
            dma((2,)),
            dma((DOWN_CHUNKS,)),
            dma((ATT_PARTS,)),
            dma((ATT_PARTS,)),
            dma((ATT_PARTS,)),
            dma((3,)),
            dma((DOWN_CHUNKS,)),
        ],
        compiler_params=pltpu.CompilerParams(
            collective_id=0, has_side_effects=True, vmem_limit_bytes=59 * 1024 * 1024
        ),
    )(
        *(
            pltpu.with_memory_space_constraint(a, pltpu.HBM)
            for a in (
                queries,
                keys_values,
                sink_logits,
                out_weight,
                expert_tokens,
                norm_gain.reshape(1, width),
                routes.T,
                route_weights.T,
                gate_weight,
                up_weight,
                down_weight,
            )
        )
    )
    return pl.pallas_call(
        put_out,
        out_shape=(
            jax.ShapeDtypeStruct((out_rows, width), BF16),
            jax.ShapeDtypeStruct((tokens, width), BF16),
        ),
        in_specs=[vmem, vmem],
        out_specs=(pl.BlockSpec(memory_space=pl.ANY),) * 2,
        scratch_shapes=[dma((2,))],
        compiler_params=pltpu.CompilerParams(vmem_limit_bytes=1024 * 1024),
    )(*held)


def solution(mesh):
    in_specs = (
        P("ep", "tp"),
        P("ep", "tp"),
        P(),
        P(),
        P(("ep", "tp"), None),
        P(),
        P(("ep", "tp"), None),
        P(("ep", "tp"), None),
        P("ep", None, "tp"),
        P("ep", None, "tp"),
        P("ep", "tp", None),
    )
    out_specs = (P(("ep", "tp"), None), P(("ep", "tp"), None))
    return jax.shard_map(body, mesh=mesh, in_specs=in_specs, out_specs=out_specs, check_vma=False)
```

```python
import functools

import jax
import jax.numpy as jnp
from jax import lax
from jax.experimental import pallas as pl
from jax.experimental.pallas import tpu as pltpu
from jax.sharding import PartitionSpec as P

MESH = pl.DeviceIdType.MESH
HEAD_DIM = 64
WINDOW = 128
CAP = 24
SIDE = 4
STEP = 7
F32 = jnp.float32
BF16 = jnp.bfloat16
NEG_FILL = -1e30

GU_CHUNKS = 4
COLUMNS = (128,) + (256,) * 7 + (128,)
DOWN_CHUNKS = len(COLUMNS)
ATT_PARTS = 2
EARLY = 1


def kernel(
    n_ep,
    n_tp,
    q_hbm,
    kv_hbm,
    sink_hbm,
    ow_hbm,
    tok_hbm,
    gain_hbm,
    routes_hbm,
    rw_hbm,
    g_hbm,
    u_hbm,
    d_hbm,
    mix_ref,
    exp_ref,
    sink_ref,
    gain_ref,
    routes_ref,
    rw_ref,
    q_v,
    kv_v,
    ow_v,
    tok_v,
    normed_v,
    slots_v,
    comb_v,
    out_v,
    arr_v,
    gu_v,
    down_v,
    hid_v,
    back_v,
    ret_v,
    att_v,
    attin_v,
    pass_v,
    acc_v,
    part_v,
    sum_v,
    got_v,
    news_sem,
    loc_sem,
    halo_sem,
    sent_sem,
    gu_sem,
    gur_sem,
    dn_sem,
    dnr_sem,
    disp_sem,
    ret_sem,
    far_sem,
    fwd_sem,
    near_sem,
    tok_sem,
    part_sem,
):
    ep = lax.axis_index("ep")
    tp = lax.axis_index("tp")
    right = lax.rem(tp + 1, n_tp)
    left = lax.rem(tp + n_tp - 1, n_tp)
    next_ep = lax.rem(ep + 1, n_ep)
    prev_ep = lax.rem(ep + n_ep - 1, n_ep)
    rows = q_v.shape[0]
    width = tok_v.shape[2]
    parity = lax.rem(tp, 2)
    at_site = lax.rem(ep, 2) == parity
    off_site = lax.rem(ep, 2) != parity
    partner = jnp.where(at_site, right, left)
    served = n_ep // 2
    place = ep // 2
    half = width // 2
    hid = gu_v.shape[3]
    starts = [sum(COLUMNS[:c]) for c in range(DOWN_CHUNKS)]
    slot_rows = 2 * n_ep * CAP
    table_rows = served * CAP

    def of_width(c):
        return pl.ds(starts[c], COLUMNS[c])

    def local(src, dst, k):
        return pltpu.make_async_copy(src, dst, loc_sem.at[k])

    loads = [
        local(tok_hbm, tok_v.at[0], 0),
        local(q_hbm, q_v, 1),
        local(kv_hbm, kv_v.at[pl.ds(WINDOW, rows)], 2),
        local(g_hbm.at[0], gu_v.at[0, 0], 3),
        local(u_hbm.at[0], gu_v.at[0, 1], 4),
        local(ow_hbm, ow_v, 5),
        local(gain_hbm, gain_ref, 6),
        local(routes_hbm, routes_ref.at[0], 7),
        local(rw_hbm, rw_ref.at[0], 8),
        local(sink_hbm, sink_ref, 9),
    ]
    for c in range(DOWN_CHUNKS):
        loads.append(local(d_hbm.at[0, :, of_width(c)], down_v.at[c, pl.ds(0, hid), pl.ds(0, COLUMNS[c])], 10))
    barrier = pltpu.get_barrier_semaphore()

    def greet(semaphore, device):
        pl.semaphore_signal(semaphore, inc=1, device_id=device, device_id_type=MESH)

    def turn(device):
        y = lax.rem(device // 2, SIDE)
        return (device // (2 * SIDE) + jnp.minimum(y, SIDE - 2)) * n_ep + device

    mine = turn(ep)
    greet(barrier, (ep, right))
    greet(barrier, (ep, left))

    def greet_later(d, count):
        to = lax.rem(ep + d, n_ep)
        later = turn(to) > mine

        @pl.when(later)
        def _():
            greet(barrier, (to, tp))

        return count + jnp.where(later, 1, 0)

    later_count = lax.fori_loop(1, n_ep, greet_later, 0)
    for copy in loads:
        copy.start()
    pl.semaphore_wait(barrier, 2 + n_ep - 1 - later_count)

    def remote(src, dst, ssem, rsem, device):
        return pltpu.make_async_remote_copy(
            src_ref=src,
            dst_ref=dst,
            send_sem=ssem,
            recv_sem=rsem,
            device_id=device,
            device_id_type=MESH,
        )

    def take(like, semaphore):
        pltpu.make_async_copy(like, like, semaphore).wait()

    def both_ways(send, p):
        for side in range(2):
            send(side, p).start()

    halos = [
        remote(
            kv_hbm.at[pl.ds(rows - WINDOW, WINDOW)],
            kv_v.at[pl.ds(0, WINDOW)],
            halo_sem.at[0],
            halo_sem.at[1],
            (next_ep, tp),
        ),
        remote(
            kv_hbm.at[pl.ds(0, WINDOW)],
            kv_v.at[pl.ds(WINDOW + rows, WINDOW)],
            halo_sem.at[0],
            halo_sem.at[1],
            (prev_ep, tp),
        ),
    ]
    def gu_own(side, k):
        which = k % 2
        part = (k // 2 + side) % 2
        src = (g_hbm, u_hbm)[which].at[0, pl.ds(part * half, half)]
        dst = gu_v.at[1 + side, which, pl.ds(part * half, half)]
        return remote(
            src, dst, sent_sem.at[0], gu_sem.at[k], (ep, (right, left)[side])
        )

    def gu_relay(side, k):
        src = gu_v.at[1 + side, k, pl.ds(side * half, half)]
        dst = gu_v.at[3, k, pl.ds(side * half, half)]
        return remote(
            src, dst, sent_sem.at[1], gur_sem.at[k], (ep, (right, left)[side])
        )

    def dn_own(side, c):
        src = d_hbm.at[0, :, of_width(c)]
        dst = down_v.at[c, pl.ds((1 + side) * hid, hid), pl.ds(0, COLUMNS[c])]
        return remote(
            src, dst, sent_sem.at[2], dn_sem.at[c], (ep, (right, left)[side])
        )

    def dn_half(side, c):
        at = side * (hid // 2)
        src = d_hbm.at[0, pl.ds(at, hid // 2), of_width(c)]
        dst = down_v.at[c, pl.ds((1 + side) * hid + at, hid // 2), pl.ds(0, COLUMNS[c])]
        return remote(src, dst, sent_sem.at[2], dn_sem.at[c], (ep, (right, left)[side]))

    def dn_relay(side, c):
        at = side * (hid // 2)
        src = down_v.at[c, pl.ds((1 + side) * hid + at, hid // 2), pl.ds(0, COLUMNS[c])]
        dst = down_v.at[c, pl.ds(3 * hid + at, hid // 2), pl.ds(0, COLUMNS[c])]
        return remote(
            src, dst, sent_sem.at[3], dnr_sem.at[c], (ep, (right, left)[side])
        )

    opposite = lax.rem(tp + 2, n_tp)
    part_rows = att_v.shape[1] // ATT_PARTS
    part_cols = att_v.shape[2] // 2

    def att_far(side, p):
        at = pl.ds(p * part_rows, part_rows)
        src = att_v.at[opposite, at, pl.ds(side * part_cols, part_cols)]
        dst = pass_v.at[side, p]
        return remote(
            src, dst, sent_sem.at[4], far_sem.at[p], (ep, (right, left)[side])
        )

    def att_fwd(side, p):
        at = pl.ds(p * part_rows, part_rows)
        dst = attin_v.at[(left, right)[side], at, pl.ds(side * part_cols, part_cols)]
        return remote(
            pass_v.at[side, p],
            dst,
            sent_sem.at[5],
            fwd_sem.at[p],
            (ep, (right, left)[side]),
        )

    def att_near(side, p):
        at = pl.ds(p * part_rows, part_rows)
        to = (right, left)[side]
        return remote(
            att_v.at[to, at], attin_v.at[tp, at], sent_sem.at[6], near_sem.at[p], (ep, to)
        )

    exchange = [
        remote(routes_hbm, routes_ref.at[1], sent_sem.at[8], tok_sem.at[0], (ep, partner)),
        remote(rw_hbm, rw_ref.at[1], sent_sem.at[9], tok_sem.at[1], (ep, partner)),
        remote(tok_hbm, tok_v.at[1], sent_sem.at[10], tok_sem.at[2], (ep, partner)),
    ]
    for copy in exchange:
        copy.start()
    @pl.loop(1, n_ep)
    def _(d):
        to = lax.rem(ep + d, n_ep)

        @pl.when(turn(to) < mine)
        def _():
            greet(news_sem, (to, tp))

    tokens = tok_v.shape[1]
    per_block = 8 * CAP

    def slot_expert(shape, axis):
        slot = lax.broadcasted_iota(jnp.int32, shape, axis).astype(F32)
        expert = jnp.floor((slot + 0.5) * (1.0 / CAP))
        return expert, slot - expert * CAP

    def tables(b):
        @pl.loop(0, 8)
        def _(i):
            at = pl.ds(pl.multiple_of(i * 32, 32), 32)
            x = tok_v[b, at, :].astype(F32)
            x = x - jnp.mean(x, -1, keepdims=True)
            var = jnp.mean(x * x, -1, keepdims=True)
            normed_v[b, at, :] = (x * lax.rsqrt(var + 1e-06) * gain_ref[...]).astype(BF16)

        expert_ids = lax.broadcasted_iota(jnp.int32, (served, tokens), 0) * 2 + parity
        is_first = expert_ids == routes_ref[b, 0:1, :]
        is_second = expert_ids == routes_ref[b, 1:2, :]
        named = is_first | is_second
        before = (
            lax.broadcasted_iota(jnp.int32, (tokens, tokens), 0)
            < lax.broadcasted_iota(jnp.int32, (tokens, tokens), 1)
        ).astype(F32)
        rank = jnp.dot(
            named.astype(F32).astype(BF16), before.astype(BF16), preferred_element_type=F32
        )
        rank = jnp.where(named, rank, -1.0)
        weight = jnp.where(is_first, rw_ref[b, 0:1, :], 0.0) + jnp.where(
            is_second, rw_ref[b, 1:2, :], 0.0
        )

        expert, _ = slot_expert((table_rows, served), 0)
        spread = (
            expert == lax.broadcasted_iota(jnp.int32, (table_rows, served), 1).astype(F32)
        ).astype(F32)
        _, place_t = slot_expert((table_rows, tokens), 0)
        ranks = jnp.dot(spread.astype(BF16), rank.astype(BF16), preferred_element_type=F32)
        slots_v[b] = jnp.where(ranks == place_t, 1.0, 0.0).astype(BF16)

        @pl.loop(0, table_rows // per_block)
        def _(i):
            at = pl.ds(pl.multiple_of(i * per_block, per_block), per_block)
            picked = jnp.dot(slots_v[b, at, :], normed_v[b], preferred_element_type=F32)
            out_v[pl.ds(i * 8, 8), b] = picked.astype(BF16).reshape(8, CAP, width)

        return rank, weight

    def dispatch(b):
        @pl.loop(0, served)
        def _(d):
            expert = lax.rem(place + d * STEP, served)
            to = expert * 2 + parity

            @pl.when(to != ep)
            def _():
                remote(
                    out_v.at[expert, b], arr_v.at[ep, b], sent_sem.at[11 + b], disp_sem.at[b], (to, tp)
                ).start()

        @pl.when(at_site)
        def _():
            arr_v[ep, b] = out_v[place, b]

    def combine_table(b, rank, weight):
        expert_c, _ = slot_expert((served, table_rows), 1)
        spread_t = (
            expert_c == lax.broadcasted_iota(jnp.int32, (served, table_rows), 0).astype(F32)
        ).astype(F32).astype(BF16)

        def over_slots(table):
            return jnp.dot(table.T.astype(BF16), spread_t, preferred_element_type=F32)

        _, place_c = slot_expert((tokens, table_rows), 1)
        chosen = over_slots(rank) == place_c
        weight_hi = weight.astype(BF16).astype(F32)
        comb_v[b, 0] = jnp.where(chosen, over_slots(weight_hi), 0.0).astype(BF16)
        comb_v[b, 1] = jnp.where(chosen, over_slots(weight - weight_hi), 0.0).astype(BF16)

    loads[0].wait()
    for k in range(6, 10):
        loads[k].wait()
    own_tables = tables(0)

    @pl.when(later_count > 0)
    def _():
        pl.semaphore_wait(news_sem, later_count)

    for copy in halos:
        copy.start()
    dispatch(0)

    combine_table(0, *own_tables)

    loads[1].wait()
    loads[2].wait()
    block = 128
    span = block + 2 * WINDOW
    heads = q_v.shape[1] // HEAD_DIM
    blocks_per_dest = rows // block // n_tp
    rel = lax.broadcasted_iota(jnp.int32, (block, span), 1) - lax.broadcasted_iota(
        jnp.int32, (block, span), 0
    )
    key_at = lax.broadcasted_iota(jnp.int32, (block, span), 1)
    seq_total = rows * n_ep

    def attend(b):
        row = pl.multiple_of(b * block, block)
        q = q_v[pl.ds(row, block), :] * jnp.asarray(HEAD_DIM**-0.5, BF16)
        kv = kv_v[pl.ds(row, span), :]
        keys = kv[:, 0:HEAD_DIM]
        values = kv[:, HEAD_DIM : 2 * HEAD_DIM]
        key_pos = key_at + (ep * rows + row - WINDOW)
        allowed = (rel >= 0) & (rel <= 2 * WINDOW) & (key_pos >= 0) & (key_pos < seq_total)
        outs = []
        for h in range(heads):
            sink = sink_ref[tp * heads + h]
            scores = lax.dot_general(
                q[:, h * HEAD_DIM : (h + 1) * HEAD_DIM],
                keys,
                (((1,), (1,)), ((), ())),
                preferred_element_type=F32,
            )
            scores = jnp.where(allowed, scores, NEG_FILL)
            top = jnp.maximum(jnp.max(scores, -1, keepdims=True), sink)
            expo = jnp.exp(scores - top)
            denom = jnp.sum(expo, -1, keepdims=True) + jnp.exp(sink - top)
            mixed = jnp.dot(expo.astype(BF16), values, preferred_element_type=F32)
            outs.append((mixed / denom).astype(BF16))
        att_v[b // blocks_per_dest, pl.ds(pl.multiple_of(lax.rem(b, blocks_per_dest) * block, block), block), :] = (
            jnp.concatenate(outs, axis=1)
        )

    blocks = rows // block

    @pl.loop(1, 3)
    def _(b):
        attend(b)

    for k in range(2):
        both_ways(gu_own, k)

    @pl.when(off_site)
    def _():
        for k in range(2, GU_CHUNKS):
            both_ways(gu_own, k)

    @pl.when(at_site)
    def _():
        for c in range(EARLY):
            both_ways(dn_half, c)

    attend(3)
    for copy in exchange:
        copy.wait_recv()
    partner_tables = tables(1)
    dispatch(1)
    combine_table(1, *partner_tables)

    @pl.loop(4, blocks - 1)
    def _(b):
        attend(b)

    halo_like = kv_v.at[pl.ds(0, 2 * WINDOW)]
    take(halo_like, halo_sem.at[1])

    @pl.loop(0, 2)
    def _(i):
        attend(i * (blocks - 1))

    def send_attended():
        for send in (att_far, att_near):
            for p in range(ATT_PARTS):
                both_ways(send, p)

    @pl.when(off_site)
    def _():
        for k in range(2):
            take(gu_v.at[1, 0], gu_sem.at[k])
            both_ways(gu_relay, k)
        for c in range(DOWN_CHUNKS):
            both_ways(dn_own, c)
            take(down_v.at[c, pl.ds(0, hid), pl.ds(0, COLUMNS[c])], dn_sem.at[c])
            both_ways(dn_relay, c)
        send_attended()

    big_block = 16 * CAP
    slot_blocks = slot_rows // big_block

    def sources(i):
        return pl.ds(lax.rem(i, 2) * 16, 16)

    def arrived(i):
        return arr_v[sources(i), i // 2].reshape(big_block, width)

    def silu_cols(i):
        return pl.ds(pl.multiple_of(i * hid, hid), hid)

    def rows_of(i):
        return pl.ds(pl.multiple_of(i * big_block, big_block), big_block)

    def widen(s, first=0, last=slot_blocks):
        @pl.loop(first, last)
        def _(i):
            x = arrived(i)
            g = jnp.dot(x, gu_v[s, 0], preferred_element_type=F32)
            u = jnp.dot(x, gu_v[s, 1], preferred_element_type=F32)
            at = rows_of(i)
            hid_v[s, at, :] = (g / (1.0 + jnp.exp(-g)) * u).astype(BF16)

    loads[3].wait()
    loads[4].wait()
    take(gu_v.at[0, 0], loc_sem.at[10])

    def part_copy(c):
        at = pl.ds(0, COLUMNS[c])
        return remote(
            part_v.at[c, :, at], got_v.at[c, :, at], sent_sem.at[13], part_sem.at[c], (ep, partner)
        )

    def combine(c):
        cols = COLUMNS[c]

        @pl.when(at_site)
        def _():
            take(ret_v.at[c, pl.ds(0, served - 1), :, :, pl.ds(0, cols)], ret_sem.at[c])

        @pl.when(off_site)
        def _():
            take(ret_v.at[c, :, :, :, pl.ds(0, cols)], ret_sem.at[c])

        def share(b):
            results = ret_v[c, :, b, :, 0:cols].reshape(table_rows, cols)
            return jnp.dot(comb_v[b, 0], results, preferred_element_type=F32) + jnp.dot(
                comb_v[b, 1], results, preferred_element_type=F32
            )

        part_v[c, :, 0:cols] = share(1).astype(BF16)
        part_copy(c).start()
        sum_v[c, :, 0:cols] = share(0)

    def finish(c):
        cols = COLUMNS[c]
        take(got_v.at[c, :, pl.ds(0, cols)], part_sem.at[c])
        exp_ref[:, of_width(c)] = (sum_v[c, :, 0:cols] + got_v[c, :, 0:cols].astype(F32)).astype(BF16)

    @pl.when(at_site)
    def _():
        for b in range(2):
            take(arr_v.at[pl.ds(0, n_ep - 1), b], disp_sem.at[b])
            widen(0, 2 * b, 2 * b + 2)
        for k in range(GU_CHUNKS):
            take(gu_v.at[1, 0], gu_sem.at[k])

        @pl.loop(1, 3)
        def _(s):
            widen(s)

        for c in range(EARLY, DOWN_CHUNKS):
            both_ways(dn_half, c)

        take(gu_v.at[3, 0], gur_sem.at[0])

        @pl.loop(0, slot_blocks)
        def _(i):
            g = jnp.dot(arrived(i), gu_v[3, 0], preferred_element_type=F32)
            acc_v[0:big_block, silu_cols(i)] = g / (1.0 + jnp.exp(-g))

        take(gu_v.at[3, 1], gur_sem.at[1])

        @pl.loop(0, slot_blocks)
        def _(i):
            u = jnp.dot(arrived(i), gu_v[3, 1], preferred_element_type=F32)
            at = rows_of(i)
            hid_v[3, at, :] = (acc_v[0:big_block, silu_cols(i)] * u).astype(BF16)

        for c in range(DOWN_CHUNKS):
            cols = COLUMNS[c]
            take(down_v.at[c, pl.ds(hid, 2 * hid), pl.ds(0, cols)], dn_sem.at[c])
            take(down_v.at[c, pl.ds(3 * hid, hid), pl.ds(0, cols)], dnr_sem.at[c])

            @pl.loop(0, slot_blocks)
            def _(i):
                at = rows_of(i)
                total = jnp.zeros((big_block, cols), F32)
                for s in range(4):
                    total = total + jnp.dot(
                        hid_v[s, at, :],
                        down_v[c, s * hid : (s + 1) * hid, 0:cols],
                        preferred_element_type=F32,
                    )
                back_v[c, sources(i), i // 2, :, 0:cols] = total.astype(BF16).reshape(16, CAP, cols)

            @pl.loop(1, n_ep)
            def _(d):
                to = lax.rem(ep + d * STEP, n_ep)
                remote(
                    back_v.at[c, to, :, :, pl.ds(0, cols)],
                    ret_v.at[c, place, :, :, pl.ds(0, cols)],
                    sent_sem.at[7],
                    ret_sem.at[c],
                    (to, tp),
                ).start()

            ret_v[c, place, :, :, 0:cols] = back_v[c, ep, :, :, 0:cols]
            if c == 4:
                send_attended()
            if c >= 5:
                combine(c - 5)

    @pl.when(off_site)
    def _():
        for c in range(4):
            combine(c)

    for p in range(ATT_PARTS):
        take(pass_v.at[:, p], far_sem.at[p])
        both_ways(att_fwd, p)

    loads[5].wait()
    head_cols = heads * HEAD_DIM
    mcol = mix_ref.shape[1] // 4

    def add_heads(p, sources, first):
        at = pl.ds(p * part_rows, part_rows)
        for n in range(4):
            cols = pl.ds(n * mcol, mcol)
            total = jnp.zeros((part_rows, mcol), F32) if first else acc_v[at, cols]
            for heads_of, source in sources:
                total = total + jnp.dot(
                    source[at, :],
                    ow_v[pl.ds(pl.multiple_of(heads_of * head_cols, head_cols), head_cols), cols],
                    preferred_element_type=F32,
                )
            if first:
                acc_v[at, cols] = total
            else:
                mix_ref[at, cols] = total.astype(BF16)

    def project_near(p):
        take(attin_v.at[pl.ds(0, 2), pl.ds(p * part_rows, part_rows)], near_sem.at[p])
        add_heads(p, ((left, attin_v.at[left]), (right, attin_v.at[right]), (tp, att_v.at[tp])), True)

    def project_far(p):
        take(attin_v.at[opposite, pl.ds(p * part_rows, part_rows)], fwd_sem.at[p])
        add_heads(p, ((opposite, attin_v.at[opposite]),), False)

    combine(4)
    combine(5)
    project_near(0)
    combine(6)
    project_near(1)
    for c in range(5):
        finish(c)
    combine(7)
    for p in range(ATT_PARTS):
        project_far(p)
    for c in range(5, 7):
        finish(c)
    combine(8)

    take(kv_v.at[pl.ds(0, 2 * WINDOW)], halo_sem.at[0])
    for copy in exchange:
        copy.wait_send()

    @pl.when(at_site)
    def _():
        take(gu_v.at[0], sent_sem.at[0])
        take(gu_v.at[0, 0], sent_sem.at[2])
        for b in range(2):
            take(out_v.at[pl.ds(0, served - 1), b], sent_sem.at[11 + b])
        for c in range(DOWN_CHUNKS):
            take(back_v.at[c, pl.ds(0, n_ep - 1), :, :, pl.ds(0, COLUMNS[c])], sent_sem.at[7])

    @pl.when(off_site)
    def _():
        take(gu_v.at[pl.ds(0, 2)], sent_sem.at[0])
        take(gu_v.at[0], sent_sem.at[1])
        take(gu_v.at[0], sent_sem.at[2])
        take(gu_v.at[0, 0], sent_sem.at[3])
        for b in range(2):
            take(out_v.at[:, b], sent_sem.at[11 + b])

    take(attin_v.at[0], sent_sem.at[4])
    take(attin_v.at[0], sent_sem.at[5])
    take(attin_v.at[pl.ds(0, 2)], sent_sem.at[6])
    finish(7)
    finish(8)
    take(normed_v.at[0], sent_sem.at[13])


def put_out(mix_ref, exp_ref, mix_hbm, exp_hbm, sem):
    copies = [
        pltpu.make_async_copy(mix_ref, mix_hbm, sem.at[0]),
        pltpu.make_async_copy(exp_ref, exp_hbm, sem.at[1]),
    ]
    for copy in copies:
        copy.start()
    for copy in copies:
        copy.wait()


def body(
    queries,
    keys_values,
    sink_logits,
    out_weight,
    expert_tokens,
    norm_gain,
    routes,
    route_weights,
    gate_weight,
    up_weight,
    down_weight,
):
    n_ep = lax.axis_size("ep")
    n_tp = lax.axis_size("tp")
    rows, q_cols = queries.shape
    tokens, width = expert_tokens.shape
    hid = gate_weight.shape[2]
    out_rows = rows // n_tp
    dcol = max(COLUMNS)
    served = n_ep // 2
    slot_rows = 2 * n_ep * CAP
    table_rows = served * CAP
    hbm = pl.BlockSpec(memory_space=pltpu.HBM)
    vmem = pl.BlockSpec(memory_space=pltpu.VMEM)
    dma = pltpu.SemaphoreType.DMA
    held = pl.pallas_call(
        functools.partial(kernel, n_ep, n_tp),
        out_shape=(
            pltpu.VMEM((out_rows, width), BF16),
            pltpu.VMEM((tokens, width), BF16),
        ),
        in_specs=[hbm] * 11,
        out_specs=(vmem, vmem),
        scratch_shapes=[
            pltpu.SMEM(sink_logits.shape, F32),
            pltpu.VMEM((1, width), F32),
            pltpu.VMEM((2, 2, tokens), jnp.int32),
            pltpu.VMEM((2, 2, tokens), F32),
            pltpu.VMEM((rows, q_cols), BF16),
            pltpu.VMEM((rows + 2 * WINDOW, 2 * HEAD_DIM), BF16),
            pltpu.VMEM(out_weight.shape, BF16),
            pltpu.VMEM((2, tokens, width), BF16),
            pltpu.VMEM((2, tokens, width), BF16),
            pltpu.VMEM((2, table_rows, tokens), BF16),
            pltpu.VMEM((2, 2, tokens, table_rows), BF16),
            pltpu.VMEM((served, 2, CAP, width), BF16),
            pltpu.VMEM((n_ep, 2, CAP, width), BF16),
            pltpu.VMEM((4, 2, width, hid), BF16),
            pltpu.VMEM((DOWN_CHUNKS, 4 * hid, dcol), BF16),
            pltpu.VMEM((4, slot_rows, hid), BF16),
            pltpu.VMEM((DOWN_CHUNKS, n_ep, 2, CAP, dcol), BF16),
            pltpu.VMEM((DOWN_CHUNKS, served, 2, CAP, dcol), BF16),
            pltpu.VMEM((n_tp, out_rows, q_cols), BF16),
            pltpu.VMEM((n_tp, out_rows, q_cols), BF16),
            pltpu.VMEM((2, ATT_PARTS, out_rows // ATT_PARTS, q_cols // 2), BF16),
            pltpu.VMEM((out_rows, width), F32),
            pltpu.VMEM((DOWN_CHUNKS, tokens, dcol), BF16),
            pltpu.VMEM((DOWN_CHUNKS, tokens, dcol), F32),
            pltpu.VMEM((DOWN_CHUNKS, tokens, dcol), BF16),
            pltpu.SemaphoreType.REGULAR,
            dma((11,)),
            dma((2,)),
            dma((14,)),
            dma((GU_CHUNKS,)),
            dma((2,)),
            dma((DOWN_CHUNKS,)),
            dma((DOWN_CHUNKS,)),
            dma((2,)),
            dma((DOWN_CHUNKS,)),
            dma((ATT_PARTS,)),
            dma((ATT_PARTS,)),
            dma((ATT_PARTS,)),
            dma((3,)),
            dma((DOWN_CHUNKS,)),
        ],
        compiler_params=pltpu.CompilerParams(
            collective_id=0, has_side_effects=True, vmem_limit_bytes=60 * 1024 * 1024
        ),
    )(
        *(
            pltpu.with_memory_space_constraint(a, pltpu.HBM)
            for a in (
                queries,
                keys_values,
                sink_logits,
                out_weight,
                expert_tokens,
                norm_gain.reshape(1, width),
                routes.T,
                route_weights.T,
                gate_weight,
                up_weight,
                down_weight,
            )
        )
    )
    return pl.pallas_call(
        put_out,
        out_shape=(
            jax.ShapeDtypeStruct((out_rows, width), BF16),
            jax.ShapeDtypeStruct((tokens, width), BF16),
        ),
        in_specs=[vmem, vmem],
        out_specs=(pl.BlockSpec(memory_space=pl.ANY),) * 2,
        scratch_shapes=[dma((2,))],
        compiler_params=pltpu.CompilerParams(vmem_limit_bytes=1024 * 1024),
    )(*held)


def solution(mesh):
    in_specs = (
        P("ep", "tp"),
        P("ep", "tp"),
        P(),
        P(),
        P(("ep", "tp"), None),
        P(),
        P(("ep", "tp"), None),
        P(("ep", "tp"), None),
        P("ep", None, "tp"),
        P("ep", None, "tp"),
        P("ep", "tp", None),
    )
    out_specs = (P(("ep", "tp"), None), P(("ep", "tp"), None))
    return jax.shard_map(body, mesh=mesh, in_specs=in_specs, out_specs=out_specs, check_vma=False)
```
